32 devices in a mesh: sp: 8 (over z, y), tp: 4 (over x, core).
Axes of the slice: x: 2, y: 2, z: 4, core: 2. Of those that a mesh axis runs over, the one named last changes fastest.
Arguments:
- resid: bfloat16 [6144, 4096], P(('sp', 'tp')), may hold values from -80 to 80
- pool_in: bfloat16 [6144, 1024], P('sp', 'tp'), may hold values from -6 to 6
- pool_weight: bfloat16 [4, 256, 256], P('tp'), may hold values from -0.375 to 0.375
- pool_scale: float32 [1024], P('tp'), may hold values from 0.1 to 1.9
- out_weight: bfloat16 [1024, 4096], P('tp'), may hold values from -0.1875 to 0.1875
- norm_gain: float32 [4096], replicated, may hold values from 0.1 to 1.9
- route_ids: int32 [6144, 4], P(('sp', 'tp')), may hold values from 0 to 31, all different within a row; in each aligned block of 192 rows (0 to 191, 192 to 383, ...) at most 36 rows name the same one
- route_weight: float32 [6144, 4], P(('sp', 'tp')), may hold values from 0.1 to 1
- expert_gate: bfloat16 [32, 4096, 384], P('sp'), may hold values from -0.09375 to 0.09375
- expert_up: bfloat16 [32, 4096, 384], P('sp'), may hold values from -0.09375 to 0.09375
- expert_down: bfloat16 [32, 384, 4096], P('sp'), may hold values from -0.3125 to 0.3125
- shared_gate: bfloat16 [4096, 384], replicated, may hold values from -0.09375 to 0.09375
- shared_up: bfloat16 [4096, 384], replicated, may hold values from -0.09375 to 0.09375
- shared_down: bfloat16 [384, 4096], replicated, may hold values from -0.3125 to 0.3125
Outputs:
- layer_out: bfloat16 [6144, 4096], P(('sp', 'tp'))
The draws below stay inside these ranges and needn't reach their ends.
Inputs may be any that keep to these rules, and one draw needn't show every extreme that they name: `route_ids`: each row names 4 different experts. Among the rows of one device no expert is named more than 36 times, and that count is reached.
All inputs are finite; a program needn't handle non-finite values.
Results may differ from the reference program's by a relative error of at most 0.012.
Values may be sent and summed in bfloat16 or wider, within the bound.
A program may use at most 192 MiB of HBM per device.

```python
import math
import jax
import jax.numpy as jnp
import numpy as np
from jax import lax

D = 4096
POOL_WIDTH = 1024
POOL_GROUP = 256
FE = 384
FS = 384
EXPERTS = 32
TOP_K = 4
TOK_DEV = 768
TOKENS = 6144
CAP = 36
N_SP = 8
N_TP = 4


def draw_resid(key, part):
    base = jnp.clip(jax.random.normal(jax.random.fold_in(key, 11), (TOKENS, D), jnp.float32), -6.0, 6.0)
    column_scale = 0.3 * 10.0 ** jax.random.uniform(jax.random.fold_in(key, 12), (D,), jnp.float32)
    return (base * column_scale[None, :]).astype(jnp.bfloat16)


def steps_of(stream_key, shape, cuts, least, high):
    gain, own = 1.0, jax.random.fold_in(stream_key, 6)
    for position, blocks in cuts:
        steps = jnp.exp(jax.random.uniform(jax.random.fold_in(own, position), (blocks,), jnp.float32, least / len(cuts), high / len(cuts)))
        gain = gain * jnp.repeat(steps, shape[position] // blocks).reshape([-1 if axis == position else 1 for axis in range(len(shape))])
    return gain


def assign_block(key, own, number, rows, amount, top, most, lean):
    ranking = jax.random.permutation(key, amount)
    crowded, ordinary = portions_of(amount, rows * top, most, lean, True), portions_of(amount, rows * top, most, lean, False)
    places = jnp.arange(amount)

    def named(sizes, turn):
        used = int((sizes > 0).sum())
        fixed = max(1, used // 4)
        moved = fixed + (places - fixed + turn * (used - fixed)) % max(1, amount - fixed)
        return jnp.zeros((amount,), jnp.int32).at[ranking[jnp.where(places < fixed, places, moved)]].set(jnp.asarray(sizes, jnp.int32))

    sizes = jnp.where(number % 4 == 0, named(crowded, number // 4), named(ordinary, number - number // 4 - 1))
    mixed = jax.random.permutation(jax.random.fold_in(own, 3), amount)
    source_of, receiver = mixed[0:amount // 2 * 2:2], mixed[1:amount // 2 * 2:2]
    margin = jnp.minimum(sizes[source_of] - 1, most - sizes[receiver]) // 2
    margin = jnp.where((source_of == ranking[0]) | (receiver == ranking[0]) | (sizes[receiver] == 0), 0, jnp.maximum(margin, 0))
    moved = jax.random.randint(jax.random.fold_in(own, 4), (amount // 2,), 0, 1 << 20) % (margin + 1)
    sizes = sizes.at[source_of].add(-moved).at[receiver].add(moved)
    labels = jnp.searchsorted(jnp.cumsum(sizes), jnp.arange(rows * top), side="right").astype(jnp.int32)
    grid = labels.reshape(top, rows).T
    grid = grid[jax.random.permutation(jax.random.fold_in(own, 1), rows)]
    turn = jax.random.randint(jax.random.fold_in(own, 2), (rows, 1), 0, top)
    return jnp.take_along_axis(grid, (jnp.arange(top)[None, :] + turn) % top, axis=1)


def portions_of(number_of, total, bound, lean, full):
    loads = [(1 << 20) // math.isqrt(standing ** lean) + 1 for standing in range(1, number_of + 1)]
    largest = bound if full else min(bound, max(-(-total // number_of), total * loads[0] // sum(loads)))
    least = 1 if total - largest >= number_of - 1 else 0
    given, spare = [largest] + [least] * (number_of - 1), total - largest - least * (number_of - 1)
    while spare > 0:
        candidates = [i for i in range(1, number_of) if given[i] < largest] or [i for i in range(1, number_of) if given[i] < bound]
        whole, budget = sum([loads[i] for i in candidates]), spare
        for i in candidates:
            extra = min(bound - given[i], max(1, budget * loads[i] // whole), spare)
            given[i] = given[i] + extra
            spare = spare - extra
    return np.array(given)


def noise(stream_key, shape, scale, bound, shards=(), held_as=jnp.bfloat16):
    loudness = steps_of(stream_key, shape, shards, -0.22, 0.18) if shards else 1.0
    values = jax.random.normal(stream_key, shape, jnp.float32) * scale * loudness
    return jnp.minimum(jnp.maximum(values, -bound), bound).astype(held_as)


def setup_inputs(seed: int = 0) -> dict:
    seeds = jax.random.split(jax.random.key(seed), 15)
    resid = draw_resid(jax.random.fold_in(seeds[14], 71), 0)
    pool_in = noise(seeds[1], (TOKENS, POOL_WIDTH), 1.0, 6.0, ((0, 8), (1, 4)))
    pool_weight = noise(seeds[2], (4, POOL_GROUP, POOL_GROUP), POOL_GROUP ** -0.5, 0.375, ((0, 4),))
    pool_scale = jnp.clip(1.0 + 0.18 * jax.random.normal(seeds[3], (POOL_WIDTH,), jnp.float32), 0.1, 1.9)
    out_weight = noise(seeds[4], (POOL_WIDTH, D), POOL_WIDTH ** -0.5, 0.1875, ((0, 4),))
    norm_gain = jnp.clip(1.0 + 0.18 * jax.random.normal(seeds[5], (D,), jnp.float32), 0.1, 1.9)
    route_ids_keys = jax.random.split(jax.random.fold_in(seeds[6], 1), TOKENS // (TOK_DEV // N_TP))
    route_ids_turns = jax.random.permutation(jax.random.fold_in(seeds[6], 3), TOKENS // (TOK_DEV // N_TP))
    route_ids = jax.vmap(lambda own, number: assign_block(jax.random.fold_in(seeds[6], 2), own, number, TOK_DEV // N_TP, EXPERTS, TOP_K, CAP, 1))(route_ids_keys, route_ids_turns).reshape((TOKENS, TOP_K))
    route_weight = jnp.clip(jnp.exp(math.log(1.0) - 2.3025851 * jax.random.uniform(seeds[7], (TOKENS, TOP_K), jnp.float32) ** steps_of(seeds[7], (TOKENS, TOP_K), ((0, 32),), -0.2, 0.2)), 0.1, 1.0)
    expert_gate = noise(seeds[8], (EXPERTS, D, FE), D ** -0.5, 0.09375, ((0, 8),))
    expert_up = noise(seeds[9], (EXPERTS, D, FE), D ** -0.5, 0.09375, ((0, 8),))
    expert_down = noise(seeds[10], (EXPERTS, FE, D), FE ** -0.5, 0.3125, ((0, 8),))
    shared_gate = noise(seeds[11], (D, FS), D ** -0.5, 0.09375)
    shared_up = noise(seeds[12], (D, FS), D ** -0.5, 0.09375)
    shared_down = noise(seeds[13], (FS, D), FS ** -0.5, 0.3125)
    return {"resid": resid, "pool_in": pool_in, "pool_weight": pool_weight, "pool_scale": pool_scale, "out_weight": out_weight, "norm_gain": norm_gain, "route_ids": route_ids, "route_weight": route_weight, "expert_gate": expert_gate, "expert_up": expert_up, "expert_down": expert_down, "shared_gate": shared_gate, "shared_up": shared_up, "shared_down": shared_down}


def pool_mix(pool_in, pool_weight, pool_scale):
    whole_len = pool_in.shape[0]
    group_width = pool_weight.shape[1]
    padded = jnp.pad(pool_in.astype(jnp.float32), ((8, 8), (0, 0)))
    positions = jnp.arange(whole_len, dtype=jnp.int32)
    outputs = []
    for group_num in range(4):
        half_span = 2 ** group_num
        columns = padded[:, group_num * group_width:(group_num + 1) * group_width]
        running = jnp.zeros((whole_len, group_width), jnp.float32)
        for row_shift in range(-half_span, half_span):
            running = running + columns[8 + row_shift:8 + row_shift + whole_len]
        upper_end = jnp.minimum(positions + half_span, whole_len)
        lower_end = jnp.maximum(positions - half_span, 0)
        row_count = (upper_end - lower_end).astype(jnp.float32)
        center = columns[8:8 + whole_len]
        spread = (running / row_count[:, None] - center).astype(jnp.bfloat16)
        outputs.append(jnp.dot(spread, pool_weight[group_num], preferred_element_type=jnp.float32))
    mixed_rows = jnp.concatenate(outputs, axis=1)
    return (mixed_rows * pool_scale[None, :]).astype(jnp.bfloat16)

def reference(resid, pool_in, pool_weight, pool_scale, out_weight, norm_gain, route_ids, route_weight, expert_gate, expert_up, expert_down, shared_gate, shared_up, shared_down):
    pooled = pool_mix(pool_in, pool_weight, pool_scale)
    middle = (resid.astype(jnp.float32) + jnp.dot(pooled, out_weight, preferred_element_type=jnp.float32)).astype(jnp.bfloat16)
    middle_float = middle.astype(jnp.float32)
    square_mean = lax.optimization_barrier(jnp.mean(middle_float * middle_float, axis=1, keepdims=True))
    normed = (middle_float * lax.rsqrt(square_mean + 1e-06) * norm_gain[None, :]).astype(jnp.bfloat16)
    shared_hidden = (jax.nn.silu(jnp.dot(normed, shared_gate, preferred_element_type=jnp.float32)) * jnp.dot(normed, shared_up, preferred_element_type=jnp.float32)).astype(jnp.bfloat16)
    shared_out = jnp.dot(shared_hidden, shared_down, preferred_element_type=jnp.float32)
    tokens_all = normed.shape[0]
    top_count = route_ids.shape[1]
    flat_ids = route_ids.reshape(-1).astype(jnp.int32)
    onehot = (flat_ids[:, None] == jnp.arange(EXPERTS, dtype=jnp.int32)[None, :]).astype(jnp.int32)
    rank_in_expert = lax.optimization_barrier(jnp.sum(jnp.cumsum(onehot, axis=0) * onehot, axis=1)) - 1
    slot_width = N_SP * N_TP * CAP
    sentinel = tokens_all * top_count
    slot_table = jnp.full((EXPERTS, slot_width), sentinel, jnp.int32).at[flat_ids, rank_in_expert].set(jnp.arange(sentinel, dtype=jnp.int32))
    extended = jnp.concatenate([normed, jnp.zeros((1, normed.shape[1]), jnp.bfloat16)], axis=0)
    weight_ext = jnp.concatenate([route_weight.reshape(-1), jnp.zeros((1,), jnp.float32)], axis=0)

    def expert_step(totals, stacked):
        gate_w, up_w, down_w, entries = stacked
        token_rows = entries // top_count
        gathered = jnp.take(extended, token_rows, axis=0)
        hidden = (jax.nn.silu(jnp.dot(gathered, gate_w, preferred_element_type=jnp.float32)) * jnp.dot(gathered, up_w, preferred_element_type=jnp.float32)).astype(jnp.bfloat16)
        produced = jnp.dot(hidden, down_w, preferred_element_type=jnp.float32).astype(jnp.bfloat16)
        weights = jnp.take(weight_ext, entries)
        return (totals.at[token_rows].add(produced.astype(jnp.float32) * weights[:, None]), None)
    start_totals = jnp.zeros((tokens_all + 1, normed.shape[1]), jnp.float32)
    routed, _ = lax.scan(expert_step, start_totals, (expert_gate, expert_up, expert_down, slot_table))
    return (middle_float + shared_out + routed[:tokens_all]).astype(jnp.bfloat16)
```

```python
import functools

import jax
import jax.numpy as jnp
from jax import lax
from jax.experimental import pallas as pl
from jax.experimental.pallas import tpu as pltpu
from jax.sharding import PartitionSpec as P

reach_rows = 8
norm_eps = 1e-06
expert_slots = 36
MESH = pl.DeviceIdType.MESH


def with_halo(cells, sides, width):
    for axis, dim in sides:
        count = lax.axis_size(axis)
        ends = count - 1
        head = lax.slice_in_dim(cells, 0, width, axis=dim)
        tail = lax.slice_in_dim(cells, cells.shape[dim] - width, cells.shape[dim], axis=dim)
        cells = jnp.concatenate(
            [
                lax.ppermute(tail, axis, [(i, (i + 1) % count) for i in range(ends)]),
                cells,
                lax.ppermute(head, axis, [((i + 1) % count, i) for i in range(ends)]),
            ],
            axis=dim,
        )
    return cells


def window_means(padded, length, offset, whole_len):
    positions = offset + lax.iota(jnp.int32, length)
    running = jnp.zeros((length,) + padded.shape[1:], jnp.float32)
    averages = []
    covered = 0
    for section_num in range(4):
        half_span = 2**section_num
        for row_shift in list(range(-half_span, -covered)) + list(range(covered, half_span)):
            running = running + padded[reach_rows + row_shift : reach_rows + row_shift + length]
        covered = half_span
        upper_end = jnp.minimum(positions + half_span, whole_len)
        lower_end = jnp.maximum(positions - half_span, 0)
        row_count = (upper_end - lower_end).astype(jnp.float32)
        averages.append(running / row_count[:, None, None])
    return averages


def moe_kernel(
    length, cap, quarters,
    x, mt, wdq, gate, up, down,
    out, xbuf, mbuf, inbuf, wdp,
    wgu, wdbuf, yb, xs, mv, xr, xp, ho, hsp, hacc, hp, hr, m8, stage, total_out,
    x_send, x_recv, m_send, m_recv, y_send, y_recv, h_send, h_recv, r_send, r_recv,
    wd_send, wd_recv, w_sem, s_sem, l_sem,
):
    f32, bf16 = jnp.float32, jnp.bfloat16
    rows, width = x.shape
    local, _, inner = gate.shape
    total = local * 2 * length
    rows_y = xr.shape[0]
    pieces = r_send.shape[1]
    piece = width // pieces
    part = wdq.shape[0]
    me = lax.axis_index("sp")
    tp = lax.axis_index("tp")
    spot, side = me // 2, me % 2
    mate = me + 1 - 2 * side
    tp_core = tp + 1 - 2 * (tp % 2)
    tp_far = (tp + quarters // 2) % quarters
    last = length - 1
    has_left, has_right = spot > 0, spot < last

    def greet(device):
        pl.semaphore_signal(barrier, inc=1, device_id=device, device_id_type=MESH)

    barrier = pltpu.get_barrier_semaphore()
    greet({"sp": mate})
    greet({"tp": tp_core})
    greet({"tp": tp_far})

    @pl.when(has_left)
    def _():
        greet({"sp": me - 2})

    @pl.when(has_right)
    def _():
        greet({"sp": me + 2})

    pl.semaphore_wait(barrier, 3 + jnp.minimum(spot, 1) + jnp.minimum(last - spot, 1))

    def remote(src, dst, send, recv, device):
        return pltpu.make_async_remote_copy(
            src_ref=src, dst_ref=dst, send_sem=send, recv_sem=recv, device_id=device, device_id_type=MESH
        )

    def row_copies(way, source, src_x, src_m):
        step = 2 if way == 0 else -2
        return (
            remote(src_x, xbuf.at[source], x_send.at[way, source], x_recv.at[source], {"sp": me + step}),
            remote(src_m, mbuf.at[source], m_send.at[way, source], m_recv.at[source], {"sp": me + step}),
        )

    def forward(way, source):
        for copy in row_copies(way, source, xbuf.at[source], mbuf.at[source]):
            copy.start()

    def arrived(source):
        for copy in row_copies(0, source, xbuf.at[source], mbuf.at[source]):
            copy.wait_recv()

    @pl.when(has_right)
    def _():
        for copy in row_copies(0, spot, x, mt):
            copy.start()

    @pl.when(has_left)
    def _():
        for copy in row_copies(1, spot, x, mt):
            copy.start()

    def quarter_copy(slot):
        src = wdp.at[2] if slot == 3 else wdq
        device = {"tp": tp_far} if slot == 2 else {"tp": tp_core}
        return remote(src, wdp.at[slot], wd_send.at[slot], wd_recv.at[slot], device)

    quarter_copy(2).start()
    quarter_copy(1).start()

    gate_load = pltpu.make_async_copy(gate, wgu.at[:, :, pl.ds(0, inner)], w_sem.at[0])
    up_load = pltpu.make_async_copy(up, wgu.at[:, :, pl.ds(inner, inner)], w_sem.at[1])
    gate_load.start()
    up_load.start()

    def source_of(j):
        close = jnp.minimum(spot, last - spot)
        near = jnp.where(j % 2 == 1, spot - (j + 1) // 2, spot + j // 2)
        far = jnp.where(spot < last - spot, spot + j - close, spot - (j - close))
        return jnp.where(j <= 2 * close, near, far)

    def take_hop(hop):
        @pl.when(spot >= hop)
        def _():
            arrived(spot - hop)

            @pl.when(has_right)
            def _():
                forward(0, spot - hop)

        @pl.when(spot + hop <= last)
        def _():
            arrived(spot + hop)

            @pl.when(has_left)
            def _():
                forward(1, spot + hop)

    def slot_hits(table, e):
        place = table[:, 5 * local + e : 5 * local + e + 1]
        columns = lax.broadcasted_iota(jnp.int32, (rows, rows_y), 1).astype(f32)
        return ((place >= 0.0) & (columns == place + float(cap * e))).astype(f32)

    def weight_of(table, i):
        return table[:, i : i + 1] + table[:, 2 * local + i : 2 * local + i + 1]

    def y_copy(j):
        return remote(xr, xp.at[j % 2], y_send.at[0], y_recv.at[j % 2], {"sp": mate})

    def h_copy(j):
        return remote(hp, hr.at[j], h_send.at[0], h_recv.at[j], {"sp": mate})

    def gather_rows(j):
        source = source_of(j)

        def fetch(src_x, src_m):
            one = pltpu.make_async_copy(src_x, xs, l_sem.at[0])
            two = pltpu.make_async_copy(src_m, mv, l_sem.at[1])
            one.start()
            two.start()
            one.wait()
            two.wait()

        @pl.when(j == 0)
        def _():
            fetch(x, mt)

        @pl.when(j > 0)
        def _():
            fetch(xbuf.at[source], mbuf.at[source])
            y_copy(j - 1).wait_send()

        c = lax.broadcasted_iota(jnp.int32, (128, 128), 1)
        group = (c >= 2 * local).astype(jnp.int32) + (c >= 4 * local).astype(jnp.int32)
        i = c - 2 * local * group
        expert = jnp.where(i < local, me * local + i, mate * local + i - local)
        choose = (lax.broadcasted_iota(jnp.int32, (128, 128), 0) == group * total + expert) & (c < 6 * local)
        table = jnp.dot(mv[...], choose.astype(f32).astype(bf16), preferred_element_type=f32)
        m8[j] = table
        hits = slot_hits(table, 0)
        for e in range(1, local):
            hits = hits + slot_hits(table, e)
        hits = hits.astype(bf16)

        def columns(q, carry):
            cols = pl.ds(pl.multiple_of(q * piece, piece), piece)
            xr[:, cols] = lax.dot_general(
                hits, xs[:, cols], (((0,), (0,)), ((), ())), preferred_element_type=f32
            ).astype(bf16)
            return carry

        lax.fori_loop(0, pieces, columns, 0)
        y_copy(j).start()

    def gated(lhs, e):
        both = jnp.dot(lhs, wgu[e], preferred_element_type=f32)
        return jax.nn.silu(both[:, :inner]) * both[:, inner:]

    def own_hidden(j):
        def one(e, carry):
            table = m8[j]
            lanes = lax.broadcasted_iota(jnp.int32, table.shape, 1)
            mine = jnp.where((lanes == e) | (lanes == 2 * local + e), table, 0.0)
            weight = jnp.sum(mine, axis=1, keepdims=True)
            cols = pl.ds(pl.multiple_of(e * inner, 128), inner)
            ho[j, :, cols] = (gated(xs[...], e) * weight).astype(bf16)
            return carry

        lax.fori_loop(0, local, one, 0)

    cover = max(-(-(cap * (e + 1)) // 16) * 16 - cap * e // 16 * 16 for e in range(local))

    def mate_hidden(j):
        y_copy(j).wait_recv()
        hacc[...] = jnp.zeros_like(hacc)

        def one(e, carry):
            first = pl.multiple_of(cap * e // 16 * 16, 16)
            found = gated(xp[j % 2, pl.ds(first, cover), :], e)
            spots = lax.broadcasted_iota(jnp.int32, found.shape, 0) + first
            keep = (spots >= cap * e) & (spots < cap * (e + 1))
            hacc[pl.ds(first, cover), :] += jnp.where(keep, found, 0.0)
            return carry

        lax.fori_loop(0, local, one, 0)

        @pl.when(j > 0)
        def _():
            h_copy(j - 1).wait_send()

        hp[...] = hacc[...].astype(bf16)
        h_copy(j).start()

    deep = local * inner

    def down_copies(c, slot):
        cols = pl.ds(pl.multiple_of(c * piece, piece), piece)
        copies = [pltpu.make_async_copy(down.at[:, cols], wdbuf.at[slot, pl.ds(0, deep), :], s_sem.at[slot, 0])]
        where = (tp, tp_core, tp_far, tp + 3 - 2 * (tp % 2) - 2 * ((tp // 2) * 2))
        for n in range(quarters):
            src = wdq.at[:, cols] if n == 0 else wdp.at[n, :, cols]
            place = pl.ds(pl.multiple_of(deep + where[n] * part, 16), part)
            copies.append(pltpu.make_async_copy(src, wdbuf.at[slot, place, :], s_sem.at[slot, 1 + n]))
        return copies

    def return_copy(way, source, q):
        cols = pl.ds(pl.multiple_of(q * piece, piece), piece)
        if way == 0:
            target, device = jnp.where(spot + 1 == source, length, source), {"sp": me + 2}
        else:
            target, device = source, {"sp": me - 2}
        return remote(
            yb.at[source, :, cols], inbuf.at[target, :, cols], r_send.at[source, q], r_recv.at[target, q], device
        )

    def return_wait(slot, q):
        cols = pl.ds(pl.multiple_of(q * piece, piece), piece)
        remote(
            yb.at[0, :, cols], inbuf.at[slot, :, cols], r_send.at[0, q], r_recv.at[slot, q], {"sp": mate}
        ).wait_recv()

    def project(j):
        source = source_of(j)
        for copy in down_copies(0, 0):
            copy.start()
        h_copy(j).wait_recv()
        table = m8[j]
        for e in range(local):
            spread = jnp.dot(slot_hits(table, e).astype(bf16), hr[j], preferred_element_type=f32)
            hsp[:, e * inner : (e + 1) * inner] = (spread * weight_of(table, local + e)).astype(bf16)

        def chunk(c, carry):
            slot = c % 2

            @pl.when(c + 1 < pieces)
            def _():
                for copy in down_copies(c + 1, 1 - slot):
                    copy.start()

            for copy in down_copies(c, slot):
                copy.wait()
            cols = pl.ds(pl.multiple_of(c * piece, piece), piece)
            result = jnp.dot(ho[j], wdbuf[slot, :deep, :], preferred_element_type=f32)
            result = result + jnp.dot(hsp[...], wdbuf[slot, deep:, :], preferred_element_type=f32)
            yb[source, :, cols] = result.astype(bf16)

            @pl.when((spot == last) & (source < spot))
            def _():
                return_copy(1, source, c).start()

            @pl.when((spot == 0) & (source > spot))
            def _():
                return_copy(0, source, c).start()

            return carry

        lax.fori_loop(0, pieces, chunk, 0)

    def step(j, carry):
        @pl.when(j > 0)
        def _():
            take_hop(j)

        gather_rows(j)

        @pl.when(j == 0)
        def _():
            gate_load.wait()
            up_load.wait()

        @pl.when(j == 2)
        def _():
            quarter_copy(2).wait_recv()
            quarter_copy(3).start()

        own_hidden(j)

        @pl.when(j == 2)
        def _():
            quarter_copy(1).wait_recv()
            quarter_copy(3).wait_recv()

        @pl.when(j >= 2)
        def _():
            project(j - 1)

        mate_hidden(j)
        return carry

    lax.fori_loop(0, length, step, 0)

    def fold(slot, q, n):
        cols = pl.ds(pl.multiple_of(q * piece, piece), piece)
        copy = pltpu.make_async_copy(inbuf.at[slot, :, cols], stage.at[n], l_sem.at[n])
        copy.start()
        copy.wait()
        return stage[n].astype(f32)

    def relay(k, carry):
        def one(q, inner_carry):
            cols = pl.ds(pl.multiple_of(q * piece, piece), piece)
            source = last - k

            @pl.when((spot > last - k) & has_right)
            def _():
                return_wait(last - k, q)
                both = yb[last - k, :, cols].astype(f32) + fold(last - k, q, 0)
                yb[last - k, :, cols] = both.astype(bf16)
                return_copy(1, last - k, q).start()

            @pl.when((spot < k) & has_left)
            def _():
                return_wait(k, q)
                both = yb[k, :, cols].astype(f32) + fold(k, q, 1)
                yb[k, :, cols] = both.astype(bf16)
                return_copy(0, k, q).start()

            return inner_carry

        return lax.fori_loop(0, pieces, one, carry)

    def tail(i, carry):
        project((1 - i) * last)
        return lax.fori_loop(1 + i * (last - 1), last + i, relay, carry)

    lax.fori_loop(0, 2, tail, 0)

    def finish(q, carry):
        cols = pl.ds(pl.multiple_of(q * piece, piece), piece)
        total_out[...] = yb[spot, :, cols].astype(f32)

        @pl.when(has_right)
        def _():
            return_wait(spot, q)
            total_out[...] += fold(spot, q, 0)

        @pl.when(has_left)
        def _():
            return_wait(length, q)
            total_out[...] += fold(length, q, 1)

        copy = pltpu.make_async_copy(total_out, out.at[:, cols], l_sem.at[0])
        copy.start()
        copy.wait()
        return carry

    lax.fori_loop(0, pieces, finish, 0)

    y_copy(last).wait_send()
    h_copy(last).wait_send()
    for slot in (1, 2, 3):
        quarter_copy(slot).wait_send()

    def drain(s, carry):
        @pl.when((s <= spot) & has_right)
        def _():
            for copy in row_copies(0, s, xbuf.at[s], mbuf.at[s]):
                copy.wait_send()

        @pl.when((s >= spot) & has_left)
        def _():
            for copy in row_copies(1, s, xbuf.at[s], mbuf.at[s]):
                copy.wait_send()

        @pl.when(s != spot)
        def _():
            def one(q, inner_carry):
                return_copy(1, s, q).wait_send()
                return inner_carry

            lax.fori_loop(0, pieces, one, 0)

        return carry

    lax.fori_loop(0, length, drain, 0)


def routed_experts(normed, route_ids, route_weight, expert_gate, expert_up, expert_down, mate_quarter):
    count = lax.axis_size("sp")
    quarters = lax.axis_size("tp")
    assert count % 2 == 0 and count >= 6 and quarters == 4
    length = count // 2
    local, _, inner = expert_gate.shape
    total = local * count
    rows, width = normed.shape
    pieces = 4
    piece = width // pieces
    cap = expert_slots
    rows_y = -(-(cap * local) // 16) * 16
    table, coarse, fine, place = routing_table(route_ids, route_weight, total)
    pad = 128 - 3 * total
    mt = jnp.concatenate([coarse, fine, place, jnp.zeros((rows, pad), jnp.bfloat16)], axis=1)
    deep = local * inner
    bf16, f32 = jnp.bfloat16, jnp.float32
    dma = pltpu.SemaphoreType.DMA
    anywhere = pl.BlockSpec(memory_space=pl.ANY)
    results = pl.pallas_call(
        functools.partial(moe_kernel, length, cap, quarters),
        out_shape=[
            jax.ShapeDtypeStruct((rows, width), f32),
            jax.ShapeDtypeStruct((length, rows, width), bf16),
            jax.ShapeDtypeStruct((length, rows, 128), bf16),
            jax.ShapeDtypeStruct((length + 1, rows, width), bf16),
            jax.ShapeDtypeStruct((quarters, deep // quarters, width), bf16),
        ],
        in_specs=[anywhere] * 6,
        out_specs=[anywhere] * 5,
        scratch_shapes=[
            pltpu.VMEM((local, width, 2 * inner), bf16),
            pltpu.VMEM((2, 2 * deep, piece), bf16),
            pltpu.VMEM((length, rows, width), bf16),
            pltpu.VMEM((rows, width), bf16),
            pltpu.VMEM((rows, 128), bf16),
            pltpu.VMEM((rows_y, width), bf16),
            pltpu.VMEM((2, rows_y, width), bf16),
            pltpu.VMEM((length, rows, deep), bf16),
            pltpu.VMEM((rows, deep), bf16),
            pltpu.VMEM((rows_y, inner), f32),
            pltpu.VMEM((rows_y, inner), bf16),
            pltpu.VMEM((length, rows_y, inner), bf16),
            pltpu.VMEM((length, rows, 128), f32),
            pltpu.VMEM((2, rows, piece), bf16),
            pltpu.VMEM((rows, piece), f32),
            dma((2, length)), dma((length,)), dma((2, length)), dma((length,)),
            dma((1,)), dma((2,)), dma((1,)), dma((length,)),
            dma((length, pieces)), dma((length + 1, pieces)),
            dma((4,)), dma((4,)), dma((2,)), dma((2, 1 + quarters)), dma((2,)),
        ],
        compiler_params=pltpu.CompilerParams(
            collective_id=0, has_side_effects=True, vmem_limit_bytes=67043328
        ),
    )(normed, mt, mate_quarter, expert_gate, expert_up, expert_down.reshape(deep, width))
    return results[0]


def routing_table(route_ids, route_weight, total):
    rows = route_ids.shape[0]
    names = lax.iota(jnp.int32, total)
    named = route_ids[:, :, None] == names[None, None, :]
    table = jnp.sum(jnp.where(named, route_weight[:, :, None], 0.0), axis=1)
    member = jnp.any(named, axis=1)
    before = (lax.iota(jnp.int32, rows)[:, None] > lax.iota(jnp.int32, rows)[None, :]).astype(jnp.bfloat16)
    rank = jnp.dot(before, member.astype(jnp.bfloat16), preferred_element_type=jnp.float32)
    place = jnp.where(member, rank, -1.0).astype(jnp.bfloat16)
    coarse = table.astype(jnp.bfloat16)
    fine = (table - coarse.astype(jnp.float32)).astype(jnp.bfloat16)
    return table, coarse, fine, place


def shards(
    resid,
    pool_in,
    pool_weight,
    pool_scale,
    out_weight,
    norm_gain,
    route_ids,
    route_weight,
    expert_gate,
    expert_up,
    expert_down,
    shared_gate,
    shared_up,
    shared_down,
):
    tok_local = pool_in.shape[0]
    count = lax.axis_size("sp")
    width = expert_down.shape[2]
    part = expert_down.shape[0] * expert_down.shape[1] // lax.axis_size("tp")
    my_quarter = lax.dynamic_slice_in_dim(
        expert_down.reshape(-1, width), lax.axis_index("tp") * part, part, axis=0
    )
    mate_quarter = lax.ppermute(my_quarter, "sp", [(i, i ^ 1) for i in range(count)])
    local_groups = pool_weight.shape[0]
    group_width = pool_weight.shape[1]
    seq_total = tok_local * lax.axis_size("sp")
    padded = with_halo(pool_in, (("sp", 0),), reach_rows)
    padded = padded.astype(jnp.float32).reshape(
        tok_local + 2 * reach_rows, local_groups, group_width
    )
    averages = window_means(padded, tok_local, lax.axis_index("sp") * tok_local, seq_total)
    center = padded[reach_rows : reach_rows + tok_local]
    group_ids = lax.axis_index("tp") * local_groups + lax.iota(jnp.int32, local_groups)
    chosen = averages[0]
    for section_num in range(1, 4):
        chosen = jnp.where((group_ids == section_num)[None, :, None], averages[section_num], chosen)
    spread = (chosen - center).astype(jnp.bfloat16)
    mixed_rows = jnp.einsum("tgc,gce->tge", spread, pool_weight, preferred_element_type=jnp.float32)
    pooled = (mixed_rows.reshape(tok_local, -1) * pool_scale[None, :]).astype(jnp.bfloat16)
    token_pooled = lax.all_to_all(pooled, "tp", split_axis=0, concat_axis=1, tiled=True)
    branch = jnp.dot(
        token_pooled,
        lax.all_gather(out_weight, "tp", axis=0, tiled=True),
        preferred_element_type=jnp.float32,
    )
    middle = (resid.astype(jnp.float32) + branch).astype(jnp.bfloat16)
    middle_float = middle.astype(jnp.float32)
    square_mean = jnp.mean(middle_float * middle_float, axis=1, keepdims=True)
    normed = (middle_float * lax.rsqrt(square_mean + norm_eps) * norm_gain[None, :]).astype(
        jnp.bfloat16
    )
    shared_hidden = (
        jax.nn.silu(jnp.dot(normed, shared_gate, preferred_element_type=jnp.float32))
        * jnp.dot(normed, shared_up, preferred_element_type=jnp.float32)
    ).astype(jnp.bfloat16)
    shared_out = jnp.dot(shared_hidden, shared_down, preferred_element_type=jnp.float32)
    routed = routed_experts(
        normed, route_ids, route_weight, expert_gate, expert_up, expert_down, mate_quarter
    )
    return (middle_float + shared_out + routed).astype(jnp.bfloat16)


def solution(mesh):
    return jax.shard_map(
        shards,
        mesh=mesh,
        in_specs=(
            P(("sp", "tp"), None),
            P("sp", "tp"),
            P("tp", None, None),
            P("tp"),
            P("tp", None),
            P(),
            P(("sp", "tp"), None),
            P(("sp", "tp"), None),
            P("sp", None, None),
            P("sp", None, None),
            P("sp", None, None),
            P(),
            P(),
            P(),
        ),
        out_specs=P(("sp", "tp"), None),
        check_vma=False,
    )
```

```python
import functools
import math

import jax
import jax.numpy as jnp
from jax import lax
from jax.experimental import pallas as pl
from jax.experimental.pallas import tpu as pltpu
from jax.sharding import PartitionSpec as P

reach_rows = 8
norm_eps = 1e-06
expert_slots = 36
MESH = pl.DeviceIdType.MESH


def with_halo(cells, sides, width):
    for axis, dim in sides:
        count = lax.axis_size(axis)
        ends = count - 1
        head = lax.slice_in_dim(cells, 0, width, axis=dim)
        tail = lax.slice_in_dim(cells, cells.shape[dim] - width, cells.shape[dim], axis=dim)
        cells = jnp.concatenate(
            [
                lax.ppermute(tail, axis, [(i, (i + 1) % count) for i in range(ends)]),
                cells,
                lax.ppermute(head, axis, [((i + 1) % count, i) for i in range(ends)]),
            ],
            axis=dim,
        )
    return cells


def window_means(padded, length, offset, whole_len):
    positions = offset + lax.iota(jnp.int32, length)
    running = jnp.zeros((length,) + padded.shape[1:], jnp.float32)
    averages = []
    covered = 0
    for section_num in range(4):
        half_span = 2**section_num
        for row_shift in list(range(-half_span, -covered)) + list(range(covered, half_span)):
            running = running + padded[reach_rows + row_shift : reach_rows + row_shift + length]
        covered = half_span
        upper_end = jnp.minimum(positions + half_span, whole_len)
        lower_end = jnp.maximum(positions - half_span, 0)
        row_count = (upper_end - lower_end).astype(jnp.float32)
        averages.append(running / row_count[:, None, None])
    return averages


def moe_kernel(
    length, cap, quarters,
    x, mt, wdq, gate, up, down,
    out, wdp, inbuf,
    xbuf, mbuf, wgu, wdbuf, xr, xp, ho, hsp, hits, hacc, hp, hr, m8, stage, total_out,
    x_send, x_recv, m_send, m_recv, y_send, y_recv, h_send, h_recv, r_send, r_recv,
    wd_send, wd_recv, w_sem, s_sem, l_sem, own_sem,
):
    f32, bf16 = jnp.float32, jnp.bfloat16
    rows, width = x.shape
    local, _, inner = gate.shape
    deep = local * inner
    total = local * 2 * length
    rows_y = xr.shape[0]
    pieces = r_send.shape[1]
    piece = width // pieces
    chunk = wdbuf.shape[2]
    chunks = width // chunk
    part = wdq.shape[0]
    me = lax.axis_index("sp")
    tp = lax.axis_index("tp")
    spot, side = me // 2, me % 2
    mate = me + 1 - 2 * side
    tp_core = tp + 1 - 2 * (tp % 2)
    tp_far = (tp + quarters // 2) % quarters
    last = length - 1
    has_left, has_right = spot > 0, spot < last
    barrier = pltpu.get_barrier_semaphore()

    def greet(device):
        pl.semaphore_signal(barrier, inc=1, device_id=device, device_id_type=MESH)

    greet({"sp": mate})
    greet({"tp": tp_core})
    greet({"tp": tp_far})

    @pl.when(has_left)
    def _():
        greet({"sp": me - 2})

    @pl.when(has_right)
    def _():
        greet({"sp": me + 2})

    pl.semaphore_wait(barrier, 3 + jnp.minimum(spot, 1) + jnp.minimum(last - spot, 1))

    def remote(src, dst, send, recv, device):
        return pltpu.make_async_remote_copy(
            src_ref=src, dst_ref=dst, send_sem=send, recv_sem=recv, device_id=device, device_id_type=MESH
        )

    def cols_of(q):
        return pl.ds(pl.multiple_of(q * piece, piece), piece)

    def onward(way):
        return {"sp": me + 2} if way == 0 else {"sp": me - 2}

    def row_copy(way, source, q, src):
        cols = cols_of(q)
        return remote(
            src.at[:, cols], xbuf.at[source, :, cols], x_send.at[way, source, q], x_recv.at[source, q], onward(way)
        )

    def table_copy(way, source, src):
        return remote(src, mbuf.at[source], m_send.at[way, source], m_recv.at[source], onward(way))

    def each_piece(act):
        def one(q, carry):
            act(q)
            return carry

        lax.fori_loop(0, pieces, one, 0)

    def send_own(way):
        table_copy(way, spot, mt).start()
        each_piece(lambda q: row_copy(way, spot, q, x).start())

    pl.when(has_right)(lambda: send_own(0))
    pl.when(has_left)(lambda: send_own(1))

    own_rows = pltpu.make_async_copy(x, xbuf.at[spot], own_sem.at[0])
    own_table = pltpu.make_async_copy(mt, mbuf.at[spot], own_sem.at[1])
    own_rows.start()
    own_table.start()

    def quarter_copy(slot):
        src = wdp.at[2] if slot == 3 else wdq
        device = {"tp": tp_far} if slot == 2 else {"tp": tp_core}
        return remote(src, wdp.at[slot], wd_send.at[slot], wd_recv.at[slot], device)

    gate_load = pltpu.make_async_copy(gate, wgu.at[:, :, pl.ds(0, inner)], w_sem.at[0])
    up_load = pltpu.make_async_copy(up, wgu.at[:, :, pl.ds(inner, inner)], w_sem.at[1])
    gate_load.start()
    up_load.start()
    quarter_copy(2).start()
    quarter_copy(1).start()

    def source_of(j):
        close = jnp.minimum(spot, last - spot)
        near = jnp.where(j % 2 == 1, spot - (j + 1) // 2, spot + j // 2)
        far = jnp.where(spot < last - spot, spot + j - close, spot - (j - close))
        return jnp.where(j <= 2 * close, near, far)

    def take_piece(hop, q):
        def take(source, way, goes_on):
            row_copy(way, source, q, xbuf.at[source]).wait_recv()
            pl.when(goes_on)(lambda: row_copy(way, source, q, xbuf.at[source]).start())

            @pl.when(q == 0)
            def _():
                table_copy(way, source, mbuf.at[source]).wait_recv()
                pl.when(goes_on)(lambda: table_copy(way, source, mbuf.at[source]).start())

        pl.when(spot >= hop)(lambda: take(spot - hop, 0, has_right))
        pl.when(spot + hop <= last)(lambda: take(spot + hop, 1, has_left))

    def slot_hits(table, e):
        place = table[:, 5 * local + e : 5 * local + e + 1]
        columns = lax.broadcasted_iota(jnp.int32, (rows, rows_y), 1).astype(f32)
        return ((place >= 0.0) & (columns == place + float(cap * e))).astype(f32)

    def weight_of(table, i):
        return table[:, i : i + 1] + table[:, 2 * local + i : 2 * local + i + 1]

    def y_copy(j, q):
        cols = cols_of(q)
        return remote(xr.at[:, cols], xp.at[j % 2, :, cols], y_send.at[q], y_recv.at[j % 2, q], {"sp": mate})

    def h_copy(j):
        return remote(hp, hr.at[j], h_send.at[0], h_recv.at[j], {"sp": mate})

    def gather_piece(j, q):
        source = source_of(j)

        @pl.when(q == 0)
        def _():
            @pl.when(j == 0)
            def _():
                own_rows.wait()
                own_table.wait()

            c = lax.broadcasted_iota(jnp.int32, (128, 128), 1)
            group = (c >= 2 * local).astype(jnp.int32) + (c >= 4 * local).astype(jnp.int32)
            i = c - 2 * local * group
            expert = jnp.where(i < local, me * local + i, mate * local + i - local)
            choose = (lax.broadcasted_iota(jnp.int32, (128, 128), 0) == group * total + expert) & (c < 6 * local)
            table = jnp.dot(mbuf[source], choose.astype(f32).astype(bf16), preferred_element_type=f32)
            m8[j] = table
            found = slot_hits(table, 0)
            for e in range(1, local):
                found = found + slot_hits(table, e)
            hits[...] = found.astype(bf16)

        @pl.when(j > 0)
        def _():
            y_copy(j - 1, q).wait_send()

        cols = cols_of(q)
        xr[:, cols] = lax.dot_general(
            hits[...], xbuf[source, :, cols], (((0,), (0,)), ((), ())), preferred_element_type=f32
        ).astype(bf16)
        y_copy(j, q).start()

    def gated(lhs, e):
        both = jnp.dot(lhs, wgu[e], preferred_element_type=f32)
        return jax.nn.silu(both[:, :inner]) * both[:, inner:]

    def own_hidden(j, first, end):
        source = source_of(j)

        def one(e, carry):
            table = m8[j]
            lanes = lax.broadcasted_iota(jnp.int32, table.shape, 1)
            mine = jnp.where((lanes == e) | (lanes == 2 * local + e), table, 0.0)
            weight = jnp.sum(mine, axis=1, keepdims=True)
            cols = pl.ds(pl.multiple_of(e * inner, 128), inner)
            ho[jnp.minimum(j, 1), :, cols] = (gated(xbuf[source], e) * weight).astype(bf16)
            return carry

        lax.fori_loop(first, end, one, 0)

    cover = max(-(-(cap * (e + 1)) // 16) * 16 - cap * e // 16 * 16 for e in range(local))

    def mate_hidden(j):
        each_piece(lambda q: y_copy(j, q).wait_recv())
        hacc[...] = jnp.zeros_like(hacc)

        def one(e, carry):
            first = pl.multiple_of(cap * e // 16 * 16, 16)
            found = gated(xp[j % 2, pl.ds(first, cover), :], e)
            spots = lax.broadcasted_iota(jnp.int32, found.shape, 0) + first
            keep = (spots >= cap * e) & (spots < cap * (e + 1))
            hacc[pl.ds(first, cover), :] += jnp.where(keep, found, 0.0)
            return carry

        lax.fori_loop(0, local, one, 0)

        @pl.when(j > 0)
        def _():
            h_copy(j - 1).wait_send()

        hp[...] = hacc[...].astype(bf16)
        h_copy(j).start()

    def down_copies(c, slot):
        cols = pl.ds(pl.multiple_of(c * chunk, chunk), chunk)
        copies = [pltpu.make_async_copy(down.at[:, cols], wdbuf.at[slot, pl.ds(0, deep), :], s_sem.at[slot, 0])]
        where = (tp, tp_core, tp_far, tp + 3 - 2 * (tp % 2) - 2 * ((tp // 2) * 2))
        for n in range(quarters):
            src = wdq.at[:, cols] if n == 0 else wdp.at[n, :, cols]
            place = pl.ds(pl.multiple_of(deep + where[n] * part, 16), part)
            copies.append(pltpu.make_async_copy(src, wdbuf.at[slot, place, :], s_sem.at[slot, 1 + n]))
        return copies

    def load_down(c, slot):
        for copy in down_copies(c, slot):
            copy.start()

    def return_copy(way, source, q):
        cols = cols_of(q)
        target = jnp.where(spot + 1 == source, length, source) if way == 0 else source
        return remote(
            xbuf.at[source, :, cols], inbuf.at[target, :, cols], r_send.at[source, q], r_recv.at[target, q], onward(way)
        )

    def return_wait(slot, q):
        cols = cols_of(q)
        remote(
            xbuf.at[0, :, cols], inbuf.at[slot, :, cols], r_send.at[0, q], r_recv.at[slot, q], {"sp": mate}
        ).wait_recv()

    def project(j):
        source = source_of(j)
        table = m8[j]
        for e in range(local):
            spread = jnp.dot(slot_hits(table, e).astype(bf16), hr[j], preferred_element_type=f32)
            hsp[:, e * inner : (e + 1) * inner] = (spread * weight_of(table, local + e)).astype(bf16)

        @pl.when((source < spot) & has_right)
        def _():
            each_piece(lambda q: row_copy(0, source, q, xbuf.at[source]).wait_send())

        @pl.when((source > spot) & has_left)
        def _():
            each_piece(lambda q: row_copy(1, source, q, xbuf.at[source]).wait_send())

        def one(c, carry):
            slot = c % 2
            pl.when(c + 1 < chunks)(lambda: load_down(c + 1, 1 - slot))
            for copy in down_copies(c, slot):
                copy.wait()
            cols = pl.ds(pl.multiple_of(c * chunk, chunk), chunk)
            result = jnp.dot(ho[jnp.minimum(j, 1)], wdbuf[slot, :deep, :], preferred_element_type=f32)
            result = result + jnp.dot(hsp[...], wdbuf[slot, deep:, :], preferred_element_type=f32)
            xbuf[source, :, cols] = result.astype(bf16)
            ratio = chunks // pieces
            whole = c % ratio == ratio - 1

            @pl.when(whole & (spot == last) & (source < spot))
            def _():
                return_copy(1, source, c // ratio).start()

            @pl.when(whole & (spot == 0) & (source > spot))
            def _():
                return_copy(0, source, c // ratio).start()

            return carry

        lax.fori_loop(0, chunks, one, 0)

    def window(w, carry):
        def one(q, inner_carry):
            pl.when((w >= 1) & (w < length))(lambda: take_piece(w, q))
            pl.when(w < length)(lambda: gather_piece(w, q))
            j = w - 1

            @pl.when((w >= 1) & (q < 2))
            def _():
                @pl.when((w == 1) & (q == 0))
                def _():
                    gate_load.wait()
                    up_load.wait()

                half = (local + 1) // 2
                own_hidden(j, q * half, jnp.minimum((q + 1) * half, local))

            @pl.when((w >= 1) & (q == 2))
            def _():
                mate_hidden(j)

                @pl.when(w == 2)
                def _():
                    quarter_copy(2).wait_recv()
                    quarter_copy(3).start()
                    quarter_copy(1).wait_recv()
                    quarter_copy(3).wait_recv()

                pl.when(w >= 2)(lambda: load_down(0, 0))

            @pl.when((w >= 1) & (q == 3))
            def _():
                h_copy(j).wait_recv()
                pl.when(w >= 2)(lambda: project(j))

            return inner_carry

        return lax.fori_loop(0, pieces, one, carry)

    lax.fori_loop(0, length + 1, window, 0)

    def fold(slot, q, n):
        cols = cols_of(q)
        if stage is None:
            return inbuf[slot, :, cols].astype(f32)
        copy = pltpu.make_async_copy(inbuf.at[slot, :, cols], stage.at[n], l_sem.at[n])
        copy.start()
        copy.wait()
        return stage[n].astype(f32)

    def relay(k, carry):
        def hand_on(way, source, q):
            cols = cols_of(q)
            return_wait(source, q)
            both = xbuf[source, :, cols].astype(f32) + fold(source, q, way)
            xbuf[source, :, cols] = both.astype(bf16)
            return_copy(way, source, q).start()

        def one(tau, inner_carry):
            left, right = tau - (last - spot), tau - spot

            @pl.when((spot > last - k) & has_right & (left >= 0) & (left < pieces))
            def _():
                hand_on(1, last - k, left)

            @pl.when((spot < k) & has_left & (right >= 0) & (right < pieces))
            def _():
                hand_on(0, k, right)

            return inner_carry

        return lax.fori_loop(1, pieces + last, one, carry)

    lax.fori_loop(1, last, relay, 0)
    load_down(0, 0)
    project(0)
    relay(last, 0)

    def finish(q, carry):
        cols = cols_of(q)
        total_out[...] = xbuf[spot, :, cols].astype(f32)

        @pl.when(has_right)
        def _():
            return_wait(spot, q)
            total_out[...] += fold(spot, q, 0)

        @pl.when(has_left)
        def _():
            return_wait(length, q)
            total_out[...] += fold(length, q, 1)

        copy = pltpu.make_async_copy(total_out, out.at[:, cols], l_sem.at[0])
        copy.start()
        copy.wait()
        return carry

    lax.fori_loop(0, pieces, finish, 0)

    each_piece(lambda q: y_copy(last, q).wait_send())
    h_copy(last).wait_send()
    for slot in (1, 2, 3):
        quarter_copy(slot).wait_send()

    def drain_own(way):
        each_piece(lambda q: row_copy(way, spot, q, x).wait_send())

    pl.when(has_right)(lambda: drain_own(0))
    pl.when(has_left)(lambda: drain_own(1))

    def drain(s, carry):
        pl.when((s <= spot) & has_right)(lambda: table_copy(0, s, mbuf.at[s]).wait_send())
        pl.when((s >= spot) & has_left)(lambda: table_copy(1, s, mbuf.at[s]).wait_send())

        @pl.when(s != spot)
        def _():
            each_piece(lambda q: return_copy(1, s, q).wait_send())

        return carry

    lax.fori_loop(0, length, drain, 0)


def routed_experts(normed, route_ids, route_weight, expert_gate, expert_up, expert_down, mate_quarter):
    count = lax.axis_size("sp")
    quarters = lax.axis_size("tp")
    assert count % 2 == 0 and count >= 6 and quarters == 4
    length = count // 2
    local, _, inner = expert_gate.shape
    total = local * count
    rows, width = normed.shape
    pieces = 4
    piece = width // pieces
    chunk = piece // 2
    cap = expert_slots
    rows_y = -(-(cap * local) // 16) * 16
    table, coarse, fine, place = routing_table(route_ids, route_weight, total)
    pad = 128 - 3 * total
    mt = jnp.concatenate([coarse, fine, place, jnp.zeros((rows, pad), jnp.bfloat16)], axis=1)
    deep = local * inner
    bf16, f32 = jnp.bfloat16, jnp.float32
    dma = pltpu.SemaphoreType.DMA
    anywhere = pl.BlockSpec(memory_space=pl.ANY)
    landing = (length + 1, rows, width)
    direct = 2 * math.prod(landing) < 12 * 2**20
    scratch = [
        pltpu.VMEM((length, rows, width), bf16),
        pltpu.VMEM((length, rows, 128), bf16),
        pltpu.VMEM((local, width, 2 * inner), bf16),
        pltpu.VMEM((2, 2 * deep, chunk), bf16),
        pltpu.VMEM((rows_y, width), bf16),
        pltpu.VMEM((2, rows_y, width), bf16),
        pltpu.VMEM((2, rows, deep), bf16),
        pltpu.VMEM((rows, deep), bf16),
        pltpu.VMEM((rows, rows_y), bf16),
        pltpu.VMEM((rows_y, inner), f32),
        pltpu.VMEM((rows_y, inner), bf16),
        pltpu.VMEM((length, rows_y, inner), bf16),
        pltpu.VMEM((length, rows, 128), f32),
        None if direct else pltpu.VMEM((2, rows, piece), bf16),
        pltpu.VMEM((rows, piece), f32),
        dma((2, length, pieces)), dma((length, pieces)), dma((2, length)), dma((length,)),
        dma((pieces,)), dma((2, pieces)), dma((1,)), dma((length,)),
        dma((length, pieces)), dma((length + 1, pieces)),
        dma((4,)), dma((4,)), dma((2,)), dma((2, 1 + quarters)), dma((2,)), dma((2,)),
    ]
    outs = [
        jax.ShapeDtypeStruct((rows, width), f32),
        jax.ShapeDtypeStruct((quarters, deep // quarters, width), bf16),
    ]
    kernel = functools.partial(moe_kernel, length, cap, quarters)
    if direct:
        scratch.insert(0, pltpu.VMEM(landing, bf16))
        gap = 8 + 1 + 13
        scratch.remove(None)

        def body(*refs):
            return kernel(*refs[:gap], None, *refs[gap:])
    else:
        outs.append(jax.ShapeDtypeStruct(landing, bf16))
        body = kernel
    results = pl.pallas_call(
        body,
        out_shape=outs,
        in_specs=[anywhere] * 6,
        out_specs=[anywhere] * len(outs),
        scratch_shapes=scratch,
        compiler_params=pltpu.CompilerParams(
            collective_id=0, has_side_effects=True, vmem_limit_bytes=67043328
        ),
    )(normed, mt, mate_quarter, expert_gate, expert_up, expert_down.reshape(deep, width))
    return results[0]


def routing_table(route_ids, route_weight, total):
    rows = route_ids.shape[0]
    names = lax.iota(jnp.int32, total)
    named = route_ids[:, :, None] == names[None, None, :]
    table = jnp.sum(jnp.where(named, route_weight[:, :, None], 0.0), axis=1)
    member = jnp.any(named, axis=1)
    before = (lax.iota(jnp.int32, rows)[:, None] > lax.iota(jnp.int32, rows)[None, :]).astype(jnp.bfloat16)
    rank = jnp.dot(before, member.astype(jnp.bfloat16), preferred_element_type=jnp.float32)
    place = jnp.where(member, rank, -1.0).astype(jnp.bfloat16)
    coarse = table.astype(jnp.bfloat16)
    fine = (table - coarse.astype(jnp.float32)).astype(jnp.bfloat16)
    return table, coarse, fine, place


def shards(
    resid,
    pool_in,
    pool_weight,
    pool_scale,
    out_weight,
    norm_gain,
    route_ids,
    route_weight,
    expert_gate,
    expert_up,
    expert_down,
    shared_gate,
    shared_up,
    shared_down,
):
    tok_local = pool_in.shape[0]
    count = lax.axis_size("sp")
    width = expert_down.shape[2]
    part = expert_down.shape[0] * expert_down.shape[1] // lax.axis_size("tp")
    my_quarter = lax.dynamic_slice_in_dim(
        expert_down.reshape(-1, width), lax.axis_index("tp") * part, part, axis=0
    )
    mate_quarter = lax.ppermute(my_quarter, "sp", [(i, i ^ 1) for i in range(count)])
    local_groups = pool_weight.shape[0]
    group_width = pool_weight.shape[1]
    seq_total = tok_local * lax.axis_size("sp")
    padded = with_halo(pool_in, (("sp", 0),), reach_rows)
    padded = padded.astype(jnp.float32).reshape(
        tok_local + 2 * reach_rows, local_groups, group_width
    )
    averages = window_means(padded, tok_local, lax.axis_index("sp") * tok_local, seq_total)
    center = padded[reach_rows : reach_rows + tok_local]
    group_ids = lax.axis_index("tp") * local_groups + lax.iota(jnp.int32, local_groups)
    chosen = averages[0]
    for section_num in range(1, 4):
        chosen = jnp.where((group_ids == section_num)[None, :, None], averages[section_num], chosen)
    spread = (chosen - center).astype(jnp.bfloat16)
    mixed_rows = jnp.einsum("tgc,gce->tge", spread, pool_weight, preferred_element_type=jnp.float32)
    pooled = (mixed_rows.reshape(tok_local, -1) * pool_scale[None, :]).astype(jnp.bfloat16)
    token_pooled = lax.all_to_all(pooled, "tp", split_axis=0, concat_axis=1, tiled=True)
    branch = jnp.dot(
        token_pooled,
        lax.all_gather(out_weight, "tp", axis=0, tiled=True),
        preferred_element_type=jnp.float32,
    )
    middle = (resid.astype(jnp.float32) + branch).astype(jnp.bfloat16)
    middle_float = middle.astype(jnp.float32)
    square_mean = jnp.mean(middle_float * middle_float, axis=1, keepdims=True)
    normed = (middle_float * lax.rsqrt(square_mean + norm_eps) * norm_gain[None, :]).astype(
        jnp.bfloat16
    )
    shared_hidden = (
        jax.nn.silu(jnp.dot(normed, shared_gate, preferred_element_type=jnp.float32))
        * jnp.dot(normed, shared_up, preferred_element_type=jnp.float32)
    ).astype(jnp.bfloat16)
    shared_out = jnp.dot(shared_hidden, shared_down, preferred_element_type=jnp.float32)
    routed = routed_experts(
        normed, route_ids, route_weight, expert_gate, expert_up, expert_down, mate_quarter
    )
    return (middle_float + shared_out + routed).astype(jnp.bfloat16)


def solution(mesh):
    return jax.shard_map(
        shards,
        mesh=mesh,
        in_specs=(
            P(("sp", "tp"), None),
            P("sp", "tp"),
            P("tp", None, None),
            P("tp"),
            P("tp", None),
            P(),
            P(("sp", "tp"), None),
            P(("sp", "tp"), None),
            P("sp", None, None),
            P("sp", None, None),
            P("sp", None, None),
            P(),
            P(),
            P(),
        ),
        out_specs=P(("sp", "tp"), None),
        check_vma=False,
    )
```

```python
import functools
import math

import jax
import jax.numpy as jnp
from jax import lax
from jax.experimental import pallas as pl
from jax.experimental.pallas import tpu as pltpu
from jax.sharding import PartitionSpec as P

norm_eps = 1e-06
expert_slots = 36
MESH = pl.DeviceIdType.MESH


def mixer_kernel(
    length, pool_in, pool_weight, pool_scale, out_weight, resid, gain, shared_gate, shared_up, shared_down, down,
    base, normed_out, wdp,
    padded, halo, own, weight, pbuf, tokens, owf, total, res, normed, sgu, sdown,
    halo_send, halo_recv, p_send, p_recv, core_send, core_recv, far_send, far_recv,
    z_send, z_recv, o_send, o_recv, d_send, d_recv, l_sem,
):
    f32, bf16 = jnp.float32, jnp.bfloat16
    block = tokens.shape[1]
    quarters = tokens.shape[0]
    tok_local, group = own.shape
    width = out_weight.shape[1]
    half = group // 2
    pieces = far_send.shape[0]
    piece = width // pieces
    me = lax.axis_index("sp")
    tp = lax.axis_index("tp")
    count = 2 * length
    spot = me // 2
    tp_core = tp + 1 - 2 * (tp % 2)
    tp_far = (tp + quarters // 2) % quarters
    tp_other = tp + 3 - 2 * (tp % 2) - 2 * ((tp // 2) * 2)
    z_mate = me + 2 - 4 * (spot % 2)
    mate = me + 1 - 2 * (me % 2)
    inner = shared_gate.shape[1]
    part = wdp.shape[1]
    d_pieces = d_send.shape[1]
    d_piece = width // d_pieces
    mine, theirs = spot % 2, 1 - spot % 2
    has_prev, has_next = me > 0, me < count - 1
    barrier = pltpu.get_barrier_semaphore()

    def greet(device):
        pl.semaphore_signal(barrier, inc=1, device_id=device, device_id_type=MESH)

    for peer in (tp_core, tp_far, tp_other):
        greet({"tp": peer})
    greet({"sp": z_mate})
    greet({"sp": mate})
    across = me + 2 * (me % 2) - 1
    has_across = (across >= 0) & (across < count)
    pl.when(has_across)(lambda: greet({"sp": across}))
    pl.semaphore_wait(barrier, 5 + has_across.astype(jnp.int32))

    def remote(src, dst, send, recv, device):
        return pltpu.make_async_remote_copy(
            src_ref=src, dst_ref=dst, send_sem=send, recv_sem=recv, device_id=device, device_id_type=MESH
        )

    def cut(side, i):
        return pl.ds(pl.multiple_of(side * half, half), half), pl.ds(i * piece, piece)

    def to_next():
        return remote(pool_in.at[pl.ds(tok_local - 16, 16)], halo.at[0], halo_send.at[0], halo_recv.at[0], {"sp": me + 1})

    def to_prev():
        return remote(pool_in.at[pl.ds(0, 16)], halo.at[1], halo_send.at[1], halo_recv.at[1], {"sp": me - 1})

    def far_copy(i):
        r, c = cut(mine, i)
        return remote(out_weight.at[r, c], owf.at[2, r, c], far_send.at[i], far_recv.at[i], {"tp": tp_far})

    def core_copy():
        return remote(out_weight, owf.at[1], core_send.at[0], core_recv.at[0], {"tp": tp_core})

    def z_copy(side, i):
        r, c = cut(side, i)
        return remote(owf.at[2, r, c], owf.at[2, r, c], z_send.at[i], z_recv.at[i], {"sp": z_mate})

    def other_copy(side, i):
        r, c = cut(side, i)
        return remote(owf.at[2, r, c], owf.at[3, r, c], o_send.at[side, i], o_recv.at[side, i], {"tp": tp_core})

    def block_copy(b):
        return remote(pbuf.at[b], tokens.at[tp], p_send.at[b], p_recv.at[tp], {"tp": b})

    def down_copy(slot, p):
        cols = pl.ds(p * d_piece, d_piece)
        src = down.at[pl.ds(pl.multiple_of(tp * part, 8), part), cols] if slot == 0 else wdp.at[2 if slot == 3 else 0, :, cols]
        device = ({"sp": mate}, {"tp": tp_core}, {"tp": tp_far}, {"tp": tp_core})[slot]
        return remote(src, wdp.at[slot, :, cols], d_send.at[slot, p], d_recv.at[slot, p], device)

    def down_arrived(p):
        down_copy(0, p).wait_recv()
        down_copy(1, p).start()
        if p < d_pieces // 2:
            down_copy(2, p).start()

    def down_relayed(p):
        down_copy(2, p).wait_recv()
        down_copy(3, p).start()

    pl.when(has_next)(lambda: to_next().start())
    pl.when(has_prev)(lambda: to_prev().start())
    for i in range(pieces):
        far_copy(i).start()
    for p in range(d_pieces):
        down_copy(0, p).start()
    core_copy().start()
    loads = [
        pltpu.make_async_copy(pool_in, own, l_sem.at[0]),
        pltpu.make_async_copy(pool_weight.at[0], weight, l_sem.at[1]),
        pltpu.make_async_copy(out_weight, owf.at[0], l_sem.at[2]),
        pltpu.make_async_copy(resid, res, l_sem.at[3]),
        pltpu.make_async_copy(shared_gate, sgu.at[:, pl.ds(0, inner)], l_sem.at[4]),
        pltpu.make_async_copy(shared_up, sgu.at[:, pl.ds(inner, inner)], l_sem.at[5]),
        pltpu.make_async_copy(shared_down, sdown, l_sem.at[6]),
    ]
    for load in loads:
        load.start()

    zeros = jnp.zeros((16, group), f32)
    padded[0:16] = zeros
    padded[16 + tok_local : 32 + tok_local] = zeros
    loads[0].wait()
    loads[1].wait()
    padded[16 : 16 + tok_local] = own[...].astype(f32)

    @pl.when(has_prev)
    def _():
        to_next().wait_recv()
        padded[0:16] = halo[0].astype(f32)

    @pl.when(has_next)
    def _():
        to_prev().wait_recv()
        padded[16 + tok_local : 32 + tok_local] = halo[1].astype(f32)

    seq_total = tok_local * count
    for b in range(quarters):
        start = b * block
        positions = me * tok_local + start + lax.broadcasted_iota(jnp.int32, (block, group), 0)
        running = jnp.zeros((block, group), f32)
        chosen = running
        covered = 0
        for number in range(4):
            span = 2**number
            for shift in list(range(-span, -covered)) + list(range(covered, span)):
                running = running + padded[16 + start + shift : 16 + start + shift + block]
            covered = span
            held = jnp.minimum(positions + span, seq_total) - jnp.maximum(positions - span, 0)
            average = running / held.astype(f32)
            chosen = average if number == 0 else jnp.where(tp == number, average, chosen)
        spread = (chosen - padded[16 + start : 16 + start + block]).astype(bf16)
        mixed = jnp.dot(spread, weight[...], preferred_element_type=f32)
        pbuf[b] = (mixed * pool_scale[...]).astype(bf16)
        pl.when(tp != b)(lambda: block_copy(b).start())

        @pl.when(tp == b)
        def _():
            tokens[b] = pbuf[b]

    for i in range(pieces):
        far_copy(i).wait_recv()
        z_copy(mine, i).start()
        other_copy(mine, i).start()
        if i == 0:
            down_arrived(0)

    loads[2].wait()
    core_copy().wait_recv()
    loads[3].wait()

    def taken(peer):
        remote(pbuf.at[0], tokens.at[peer], p_send.at[0], p_recv.at[peer], {"tp": peer}).wait_recv()

    step = width // 4

    def add(slots, first):
        def one(q, carry):
            cols = pl.ds(pl.multiple_of(q * step, step), step)
            value = res[:, cols].astype(f32) if first else total[:, cols]
            branch = jnp.zeros_like(value) if first else value
            for slot, peer in slots:
                branch = branch + jnp.dot(tokens[peer], owf[slot, :, cols], preferred_element_type=f32)
            total[:, cols] = branch
            return carry

        lax.fori_loop(0, width // step, one, 0)

    taken(tp_core)
    add(((0, tp), (1, tp_core)), True)
    taken(tp_far)
    taken(tp_other)
    for i in range(pieces):
        z_copy(theirs, i).wait_recv()
        other_copy(theirs, i).start()
    for i in range(pieces):
        other_copy(mine, i).wait_recv()
        other_copy(theirs, i).wait_recv()
    down_arrived(1)
    add(((2, tp_far), (3, tp_other)), False)

    def square(q, carry):
        cols = pl.ds(pl.multiple_of(q * step, step), step)
        mid = (res[:, cols].astype(f32) + total[:, cols]).astype(bf16)
        res[:, cols] = mid
        wide = mid.astype(f32)
        return carry + jnp.sum(wide * wide, axis=1, keepdims=True)

    sums = lax.fori_loop(0, width // step, square, jnp.zeros((block, 1), f32))
    scale = lax.rsqrt(sums / width + norm_eps)

    def spread_norm(q, carry):
        cols = pl.ds(pl.multiple_of(q * step, step), step)
        normed[:, cols] = (res[:, cols].astype(f32) * scale * gain[:, cols]).astype(bf16)
        return carry

    lax.fori_loop(0, width // step, spread_norm, 0)
    put_normed = pltpu.make_async_copy(normed, normed_out, l_sem.at[0])
    put_normed.start()
    for load in loads[4:]:
        load.wait()
    both = jnp.dot(normed[...], sgu[...], preferred_element_type=f32)
    hidden = (jax.nn.silu(both[:, :inner]) * both[:, inner:]).astype(bf16)

    def shared(q, carry):
        cols = pl.ds(pl.multiple_of(q * step, step), step)
        total[:, cols] = res[:, cols].astype(f32) + jnp.dot(hidden, sdown[:, cols], preferred_element_type=f32)
        return carry

    lax.fori_loop(0, width // step, shared, 0)
    put_base = pltpu.make_async_copy(total, base, l_sem.at[1])
    put_base.start()
    down_relayed(0)
    down_arrived(2)
    for p in range(1, d_pieces // 2):
        down_relayed(p)
    for p in range(3, d_pieces):
        down_arrived(p)
    for p in range(d_pieces):
        down_copy(1, p).wait_recv()
        if p < d_pieces // 2:
            down_copy(3, p).wait_recv()
            down_copy(2, p).wait_send()
            down_copy(3, p).wait_send()
        down_copy(0, p).wait_send()
        down_copy(1, p).wait_send()
    put_normed.wait()
    put_base.wait()

    pl.when(has_next)(lambda: to_next().wait_send())
    pl.when(has_prev)(lambda: to_prev().wait_send())
    core_copy().wait_send()
    for i in range(pieces):
        far_copy(i).wait_send()
        z_copy(mine, i).wait_send()
        other_copy(mine, i).wait_send()
        other_copy(theirs, i).wait_send()
    for b in range(quarters):
        pl.when(tp != b)(lambda: block_copy(b).wait_send())


def mixer(pool_in, pool_weight, pool_scale, out_weight, resid, gain, shared_gate, shared_up, shared_down, down):
    count = lax.axis_size("sp")
    quarters = lax.axis_size("tp")
    length = count // 2
    tok_local, group = pool_in.shape
    assert pool_weight.shape[0] == 1 and quarters == 4 and length % 2 == 0
    rows, width = resid.shape
    bf16, f32 = jnp.bfloat16, jnp.float32
    dma = pltpu.SemaphoreType.DMA
    pieces = 2
    deep = down.shape[0]
    inner = shared_gate.shape[1]
    anywhere = pl.BlockSpec(memory_space=pl.ANY)
    local = pl.BlockSpec(memory_space=pltpu.VMEM)
    return pl.pallas_call(
        functools.partial(mixer_kernel, length),
        out_shape=[
            jax.ShapeDtypeStruct((rows, width), f32),
            jax.ShapeDtypeStruct((rows, width), bf16),
            jax.ShapeDtypeStruct((quarters, deep // quarters, width), bf16),
        ],
        in_specs=[anywhere, anywhere, local, anywhere, anywhere, local] + [anywhere] * 4,
        out_specs=[anywhere] * 3,
        scratch_shapes=[
            pltpu.VMEM((tok_local + 32, group), f32),
            pltpu.VMEM((2, 16, group), bf16),
            pltpu.VMEM((tok_local, group), bf16),
            pltpu.VMEM((group, group), bf16),
            pltpu.VMEM((quarters, rows, group), bf16),
            pltpu.VMEM((quarters, rows, group), bf16),
            pltpu.VMEM((quarters, group, width), bf16),
            pltpu.VMEM((rows, width), f32),
            pltpu.VMEM((rows, width), bf16),
            pltpu.VMEM((rows, width), bf16),
            pltpu.VMEM((width, 2 * inner), bf16),
            pltpu.VMEM((inner, width), bf16),
            dma((2,)), dma((2,)), dma((quarters,)), dma((quarters,)), dma((1,)), dma((1,)),
            dma((pieces,)), dma((pieces,)), dma((pieces,)), dma((pieces,)),
            dma((2, pieces)), dma((2, pieces)), dma((4, 4)), dma((4, 4)), dma((7,)),
        ],
        compiler_params=pltpu.CompilerParams(
            collective_id=1, has_side_effects=True, vmem_limit_bytes=56 * 2**20
        ),
        cost_estimate=pl.CostEstimate(flops=10**11, bytes_accessed=10**8, transcendentals=0),
    )(
        pool_in, pool_weight, pool_scale[None, :], out_weight, resid, gain[None, :],
        shared_gate, shared_up, shared_down, down,
    )


def moe_kernel(
    length, cap, quarters,
    x, mt, wdp_in, gate, up, down, base,
    out, wdp, inbuf,
    xbuf, mbuf, wgu, wdbuf, xr, xp, ho, hsp, hits, hacc, hp, hr, m8, stage, total_out, out_stage,
    x_send, x_recv, m_send, m_recv, y_send, y_recv, h_send, h_recv, r_send, r_recv,
    wd_send, wd_recv, w_sem, s_sem, l_sem, own_sem,
):
    f32, bf16 = jnp.float32, jnp.bfloat16
    rows, width = x.shape
    local, _, inner = gate.shape
    deep = local * inner
    total = local * 2 * length
    rows_y = xr.shape[0]
    pieces = r_send.shape[1]
    piece = width // pieces
    chunk = wdbuf.shape[2]
    chunks = width // chunk
    part = wdp.shape[1]
    me = lax.axis_index("sp")
    tp = lax.axis_index("tp")
    spot, side = me // 2, me % 2
    mate = me + 1 - 2 * side
    tp_core = tp + 1 - 2 * (tp % 2)
    tp_far = (tp + quarters // 2) % quarters
    last = length - 1
    has_left, has_right = spot > 0, spot < last
    barrier = pltpu.get_barrier_semaphore()

    def greet(device):
        pl.semaphore_signal(barrier, inc=1, device_id=device, device_id_type=MESH)

    greet({"sp": mate})
    greet({"tp": tp_core})
    greet({"tp": tp_far})

    @pl.when(has_left)
    def _():
        greet({"sp": me - 2})

    @pl.when(has_right)
    def _():
        greet({"sp": me + 2})

    pl.semaphore_wait(barrier, 3 + jnp.minimum(spot, 1) + jnp.minimum(last - spot, 1))

    def remote(src, dst, send, recv, device):
        return pltpu.make_async_remote_copy(
            src_ref=src, dst_ref=dst, send_sem=send, recv_sem=recv, device_id=device, device_id_type=MESH
        )

    def cols_of(q):
        return pl.ds(pl.multiple_of(q * piece, piece), piece)

    def onward(way):
        return {"sp": me + 2} if way == 0 else {"sp": me - 2}

    def row_copy(way, source, q, src):
        cols = cols_of(q)
        return remote(
            src.at[:, cols], xbuf.at[source, :, cols], x_send.at[way, source, q], x_recv.at[source, q], onward(way)
        )

    def table_copy(way, source, src):
        return remote(src, mbuf.at[source], m_send.at[way, source], m_recv.at[source], onward(way))

    def each_piece(act):
        def one(q, carry):
            act(q)
            return carry

        lax.fori_loop(0, pieces, one, 0)

    def send_own(way):
        table_copy(way, spot, mt).start()
        each_piece(lambda q: row_copy(way, spot, q, x).start())

    pl.when(has_right)(lambda: send_own(0))
    pl.when(has_left)(lambda: send_own(1))

    own_rows = pltpu.make_async_copy(x, xbuf.at[spot], own_sem.at[0])
    own_table = pltpu.make_async_copy(mt, mbuf.at[spot], own_sem.at[1])
    own_rows.start()
    own_table.start()

    late = width // 2

    def quarter_copy(slot):
        cols = pl.ds(late, width - late)
        src = wdp.at[0 if slot == 2 else 2, :, cols]
        device = {"tp": tp_far} if slot == 2 else {"tp": tp_core}
        return remote(src, wdp.at[slot, :, cols], wd_send.at[slot], wd_recv.at[slot], device)

    gate_load = pltpu.make_async_copy(gate, wgu.at[:, :, pl.ds(0, inner)], w_sem.at[0])
    up_load = pltpu.make_async_copy(up, wgu.at[:, :, pl.ds(inner, inner)], w_sem.at[1])
    gate_load.start()
    up_load.start()
    quarter_copy(2).start()
    base_load = pltpu.make_async_copy(base, total_out, own_sem.at[2])
    base_load.start()

    def source_of(j):
        close = jnp.minimum(spot, last - spot)
        near = jnp.where(j % 2 == 1, spot - (j + 1) // 2, spot + j // 2)
        far = jnp.where(spot < last - spot, spot + j - close, spot - (j - close))
        return jnp.where(j <= 2 * close, near, far)

    def take_piece(hop, q):
        def take(source, way, goes_on):
            row_copy(way, source, q, xbuf.at[source]).wait_recv()
            pl.when(goes_on)(lambda: row_copy(way, source, q, xbuf.at[source]).start())

            @pl.when(q == 0)
            def _():
                table_copy(way, source, mbuf.at[source]).wait_recv()
                pl.when(goes_on)(lambda: table_copy(way, source, mbuf.at[source]).start())

        pl.when(spot >= hop)(lambda: take(spot - hop, 0, has_right))
        pl.when(spot + hop <= last)(lambda: take(spot + hop, 1, has_left))

    def slot_hits(table, e):
        place = table[:, 5 * local + e : 5 * local + e + 1]
        columns = lax.broadcasted_iota(jnp.int32, (rows, rows_y), 1).astype(f32)
        return ((place >= 0.0) & (columns == place + float(cap * e))).astype(f32)

    def weight_of(table, i):
        return table[:, i : i + 1] + table[:, 2 * local + i : 2 * local + i + 1]

    def y_copy(j, q):
        cols = cols_of(q)
        return remote(xr.at[:, cols], xp.at[j % 2, :, cols], y_send.at[q], y_recv.at[j % 2, q], {"sp": mate})

    def h_copy(j):
        return remote(hp, hr.at[j], h_send.at[0], h_recv.at[j], {"sp": mate})

    def gather_piece(j, q):
        source = source_of(j)

        @pl.when(q == 0)
        def _():
            @pl.when(j == 0)
            def _():
                own_rows.wait()
                own_table.wait()

            c = lax.broadcasted_iota(jnp.int32, (128, 128), 1)
            group = (c >= 2 * local).astype(jnp.int32) + (c >= 4 * local).astype(jnp.int32)
            i = c - 2 * local * group
            expert = jnp.where(i < local, me * local + i, mate * local + i - local)
            choose = (lax.broadcasted_iota(jnp.int32, (128, 128), 0) == group * total + expert) & (c < 6 * local)
            table = jnp.dot(mbuf[source], choose.astype(f32).astype(bf16), preferred_element_type=f32)
            m8[j] = table
            found = slot_hits(table, 0)
            for e in range(1, local):
                found = found + slot_hits(table, e)
            hits[...] = found.astype(bf16)

        @pl.when(j > 0)
        def _():
            y_copy(j - 1, q).wait_send()

        cols = cols_of(q)
        xr[:, cols] = lax.dot_general(
            hits[...], xbuf[source, :, cols], (((0,), (0,)), ((), ())), preferred_element_type=f32
        ).astype(bf16)
        y_copy(j, q).start()

    def gated(lhs, e):
        both = jnp.dot(lhs, wgu[e], preferred_element_type=f32)
        return jax.nn.silu(both[:, :inner]) * both[:, inner:]

    def own_hidden(j, first, end):
        source = source_of(j)

        def one(e, carry):
            table = m8[j]
            lanes = lax.broadcasted_iota(jnp.int32, table.shape, 1)
            mine = jnp.where((lanes == e) | (lanes == 2 * local + e), table, 0.0)
            weight = jnp.sum(mine, axis=1, keepdims=True)
            cols = pl.ds(pl.multiple_of(e * inner, 128), inner)
            ho[jnp.minimum(j, 1), :, cols] = (gated(xbuf[source], e) * weight).astype(bf16)
            return carry

        lax.fori_loop(first, end, one, 0)

    cover = max(-(-(cap * (e + 1)) // 16) * 16 - cap * e // 16 * 16 for e in range(local))

    def mate_hidden(j):
        each_piece(lambda q: y_copy(j, q).wait_recv())
        hacc[...] = jnp.zeros_like(hacc)

        def one(e, carry):
            first = pl.multiple_of(cap * e // 16 * 16, 16)
            found = gated(xp[j % 2, pl.ds(first, cover), :], e)
            spots = lax.broadcasted_iota(jnp.int32, found.shape, 0) + first
            keep = (spots >= cap * e) & (spots < cap * (e + 1))
            hacc[pl.ds(first, cover), :] += jnp.where(keep, found, 0.0)
            return carry

        lax.fori_loop(0, local, one, 0)

        @pl.when(j > 0)
        def _():
            h_copy(j - 1).wait_send()

        hp[...] = hacc[...].astype(bf16)
        h_copy(j).start()

    def down_copies(c, slot):
        cols = pl.ds(pl.multiple_of(c * chunk, chunk), chunk)
        copies = [pltpu.make_async_copy(down.at[:, cols], wdbuf.at[slot, pl.ds(0, deep), :], s_sem.at[slot, 0])]
        where = (tp, tp_core, tp_far, tp + 3 - 2 * (tp % 2) - 2 * ((tp // 2) * 2))
        for n in range(quarters):
            src = wdp.at[n, :, cols]
            place = pl.ds(pl.multiple_of(deep + where[n] * part, 16), part)
            copies.append(pltpu.make_async_copy(src, wdbuf.at[slot, place, :], s_sem.at[slot, 1 + n]))
        return copies

    def load_down(c, slot):
        for copy in down_copies(c, slot):
            copy.start()

    def return_copy(way, source, q):
        cols = cols_of(q)
        target = jnp.where(spot + 1 == source, length, source) if way == 0 else source
        return remote(
            xbuf.at[source, :, cols], inbuf.at[target, :, cols], r_send.at[source, q], r_recv.at[target, q], onward(way)
        )

    def return_wait(slot, q):
        cols = cols_of(q)
        remote(
            xbuf.at[0, :, cols], inbuf.at[slot, :, cols], r_send.at[0, q], r_recv.at[slot, q], {"sp": mate}
        ).wait_recv()

    def scatter_hidden(j):
        table = m8[j]
        for e in range(local):
            spread = jnp.dot(slot_hits(table, e).astype(bf16), hr[j], preferred_element_type=f32)
            hsp[:, e * inner : (e + 1) * inner] = (spread * weight_of(table, local + e)).astype(bf16)

    ratio = chunks // pieces

    def down_chunk(j, c):
        slot = c % 2
        pl.when(c + 1 < chunks)(lambda: load_down(c + 1, 1 - slot))
        for copy in down_copies(c, slot):
            copy.wait()
        cols = pl.ds(pl.multiple_of(c * chunk, chunk), chunk)
        result = jnp.dot(ho[jnp.minimum(j, 1)], wdbuf[slot, :deep, :], preferred_element_type=f32)
        return cols, result + jnp.dot(hsp[...], wdbuf[slot, deep:, :], preferred_element_type=f32)

    def project(j, first, end):
        source = source_of(j)

        def one(c, carry):
            fresh = c % ratio == 0
            pl.when(fresh & (source < spot) & has_right)(
                lambda: row_copy(0, source, c // ratio, xbuf.at[source]).wait_send()
            )
            pl.when(fresh & (source > spot) & has_left)(
                lambda: row_copy(1, source, c // ratio, xbuf.at[source]).wait_send()
            )
            cols, result = down_chunk(j, c)
            xbuf[source, :, cols] = result.astype(bf16)
            whole = c % ratio == ratio - 1

            @pl.when(whole & (spot == last) & (source < spot))
            def _():
                return_copy(1, source, c // ratio).start()

            @pl.when(whole & (spot == 0) & (source > spot))
            def _():
                return_copy(0, source, c // ratio).start()

            return carry

        lax.fori_loop(first, end, one, 0)

    def project_own():
        load_down(0, 0)
        scatter_hidden(0)

        def one(c, carry):
            cols, result = down_chunk(0, c)
            total_out[:, cols] += result
            return carry

        lax.fori_loop(0, chunks, one, 0)

    def window(w, carry):
        j = w - 1

        @pl.when(w == 1)
        def _():
            gate_load.wait()
            up_load.wait()

        def one(q, inner_carry):
            pl.when((w >= 1) & (w < length))(lambda: take_piece(w, q))
            pl.when(w < length)(lambda: gather_piece(w, q))
            pl.when((w >= 1) & (q == 0))(lambda: own_hidden(j, 0, local))

            @pl.when((w >= 1) & (q == 1))
            def _():
                mate_hidden(j)

                @pl.when(w == 2)
                def _():
                    quarter_copy(2).wait_recv()
                    quarter_copy(3).start()
                    quarter_copy(3).wait_recv()

                pl.when(w >= 2)(lambda: load_down(0, 0))

            @pl.when((w >= 1) & (q == 2))
            def _():
                h_copy(j).wait_recv()
                pl.when(w >= 2)(lambda: scatter_hidden(j))

            @pl.when((w >= 2) & (q >= 2))
            def _():
                middle = chunks // 2
                project(j, (q - 2) * middle, (q - 1) * middle)

            return inner_carry

        return lax.fori_loop(0, pieces, one, carry)

    lax.fori_loop(0, length + 1, window, 0)

    def fold(slot, q, n):
        cols = cols_of(q)
        if stage is None:
            return inbuf[slot, :, cols].astype(f32)
        copy = pltpu.make_async_copy(inbuf.at[slot, :, cols], stage.at[n], l_sem.at[n])
        copy.start()
        copy.wait()
        return stage[n].astype(f32)

    def relay(k, carry):
        def hand_on(way, source, q):
            cols = cols_of(q)
            return_wait(source, q)
            both = xbuf[source, :, cols].astype(f32) + fold(source, q, way)
            xbuf[source, :, cols] = both.astype(bf16)
            return_copy(way, source, q).start()

        def one(tau, inner_carry):
            left, right = tau - (last - spot), tau - spot

            @pl.when((spot > last - k) & has_right & (left >= 0) & (left < pieces))
            def _():
                hand_on(1, last - k, left)

            @pl.when((spot < k) & has_left & (right >= 0) & (right < pieces))
            def _():
                hand_on(0, k, right)

            return inner_carry

        return lax.fori_loop(1, pieces + last, one, carry)

    lax.fori_loop(1, last, relay, 0)
    base_load.wait()
    project_own()
    relay(last, 0)

    def out_copy(q):
        cols = cols_of(q)
        return pltpu.make_async_copy(out_stage.at[:, cols], out.at[:, cols], s_sem.at[0, q])

    def finish(q, carry):
        cols = cols_of(q)

        @pl.when(has_right)
        def _():
            return_wait(spot, q)
            total_out[:, cols] += fold(spot, q, 0)

        @pl.when(has_left)
        def _():
            return_wait(length, q)
            total_out[:, cols] += fold(length, q, 1)

        out_stage[:, cols] = total_out[:, cols].astype(bf16)
        out_copy(q).start()
        return carry

    lax.fori_loop(0, pieces, finish, 0)
    each_piece(lambda q: out_copy(q).wait())

    each_piece(lambda q: y_copy(last, q).wait_send())
    h_copy(last).wait_send()
    for slot in (2, 3):
        quarter_copy(slot).wait_send()

    def drain_own(way):
        each_piece(lambda q: row_copy(way, spot, q, x).wait_send())

    pl.when(has_right)(lambda: drain_own(0))
    pl.when(has_left)(lambda: drain_own(1))

    def drain(s, carry):
        pl.when((s <= spot) & has_right)(lambda: table_copy(0, s, mbuf.at[s]).wait_send())
        pl.when((s >= spot) & has_left)(lambda: table_copy(1, s, mbuf.at[s]).wait_send())

        @pl.when(s != spot)
        def _():
            each_piece(lambda q: return_copy(1, s, q).wait_send())

        return carry

    lax.fori_loop(0, length, drain, 0)


def routed_experts(normed, route_ids, route_weight, expert_gate, expert_up, expert_down, mate_down, base):
    count = lax.axis_size("sp")
    quarters = lax.axis_size("tp")
    assert count % 2 == 0 and count >= 6 and quarters == 4
    length = count // 2
    local, _, inner = expert_gate.shape
    total = local * count
    rows, width = normed.shape
    pieces = 4
    piece = width // pieces
    chunk = piece // 2
    cap = expert_slots
    rows_y = -(-(cap * local) // 16) * 16
    table, coarse, fine, place = routing_table(route_ids, route_weight, total)
    pad = 128 - 3 * total
    mt = jnp.concatenate([coarse, fine, place, jnp.zeros((rows, pad), jnp.bfloat16)], axis=1)
    deep = local * inner
    bf16, f32 = jnp.bfloat16, jnp.float32
    dma = pltpu.SemaphoreType.DMA
    anywhere = pl.BlockSpec(memory_space=pl.ANY)
    landing = (length + 1, rows, width)
    direct = 2 * math.prod(landing) < 12 * 2**20
    scratch = [
        pltpu.VMEM((length, rows, width), bf16),
        pltpu.VMEM((length, rows, 128), bf16),
        pltpu.VMEM((local, width, 2 * inner), bf16),
        pltpu.VMEM((2, 2 * deep, chunk), bf16),
        pltpu.VMEM((rows_y, width), bf16),
        pltpu.VMEM((2, rows_y, width), bf16),
        pltpu.VMEM((2, rows, deep), bf16),
        pltpu.VMEM((rows, deep), bf16),
        pltpu.VMEM((rows, rows_y), bf16),
        pltpu.VMEM((rows_y, inner), f32),
        pltpu.VMEM((rows_y, inner), bf16),
        pltpu.VMEM((length, rows_y, inner), bf16),
        pltpu.VMEM((length, rows, 128), f32),
        None if direct else pltpu.VMEM((2, rows, piece), bf16),
        pltpu.VMEM((rows, width), f32),
        pltpu.VMEM((rows, width), bf16),
        dma((2, length, pieces)), dma((length, pieces)), dma((2, length)), dma((length,)),
        dma((pieces,)), dma((2, pieces)), dma((1,)), dma((length,)),
        dma((length, pieces)), dma((length + 1, pieces)),
        dma((4,)), dma((4,)), dma((2,)), dma((2, 1 + quarters)), dma((2,)), dma((3,)),
    ]
    outs = [
        jax.ShapeDtypeStruct((rows, width), bf16),
        jax.ShapeDtypeStruct((quarters, deep // quarters, width), bf16),
    ]
    kernel = functools.partial(moe_kernel, length, cap, quarters)
    if direct:
        scratch.insert(0, pltpu.VMEM(landing, bf16))
        gap = 9 + 1 + 13
        scratch.remove(None)

        def body(*refs):
            return kernel(*refs[:gap], None, *refs[gap:])
    else:
        outs.append(jax.ShapeDtypeStruct(landing, bf16))
        body = kernel
    results = pl.pallas_call(
        body,
        out_shape=outs,
        in_specs=[anywhere] * 7,
        out_specs=[anywhere] * len(outs),
        input_output_aliases={2: 1},
        scratch_shapes=scratch,
        compiler_params=pltpu.CompilerParams(
            collective_id=0, has_side_effects=True, vmem_limit_bytes=67043328
        ),
    )(normed, mt, mate_down, expert_gate, expert_up, expert_down.reshape(deep, width), base)
    return results[0]


def routing_table(route_ids, route_weight, total):
    rows = route_ids.shape[0]
    names = lax.iota(jnp.int32, total)
    named = route_ids[:, :, None] == names[None, None, :]
    table = jnp.sum(jnp.where(named, route_weight[:, :, None], 0.0), axis=1)
    member = jnp.any(named, axis=1)
    before = (lax.iota(jnp.int32, rows)[:, None] > lax.iota(jnp.int32, rows)[None, :]).astype(jnp.bfloat16)
    rank = jnp.dot(before, member.astype(jnp.bfloat16), preferred_element_type=jnp.float32)
    place = jnp.where(member, rank, -1.0).astype(jnp.bfloat16)
    coarse = table.astype(jnp.bfloat16)
    fine = (table - coarse.astype(jnp.float32)).astype(jnp.bfloat16)
    return table, coarse, fine, place


def shards(
    resid,
    pool_in,
    pool_weight,
    pool_scale,
    out_weight,
    norm_gain,
    route_ids,
    route_weight,
    expert_gate,
    expert_up,
    expert_down,
    shared_gate,
    shared_up,
    shared_down,
):
    flat_down = expert_down.reshape(-1, expert_down.shape[2])
    base, normed, mate_down = mixer(
        pool_in, pool_weight, pool_scale, out_weight, resid, norm_gain, shared_gate, shared_up, shared_down, flat_down
    )
    return routed_experts(
        normed, route_ids, route_weight, expert_gate, expert_up, expert_down, mate_down, base
    )


def solution(mesh):
    return jax.shard_map(
        shards,
        mesh=mesh,
        in_specs=(
            P(("sp", "tp"), None),
            P("sp", "tp"),
            P("tp", None, None),
            P("tp"),
            P("tp", None),
            P(),
            P(("sp", "tp"), None),
            P(("sp", "tp"), None),
            P("sp", None, None),
            P("sp", None, None),
            P("sp", None, None),
            P(),
            P(),
            P(),
        ),
        out_specs=P(("sp", "tp"), None),
        check_vma=False,
    )
```

```python
import functools
import math

import jax
import jax.numpy as jnp
from jax import lax
from jax.experimental import pallas as pl
from jax.experimental.pallas import tpu as pltpu
from jax.sharding import PartitionSpec as P

norm_eps = 1e-06
expert_slots = 36
MESH = pl.DeviceIdType.MESH


def mixer_kernel(
    length, pool_in, pool_weight, pool_scale, out_weight, resid, gain, shared_gate, shared_up, shared_down, down,
    base, normed_out, wdp,
    padded, halo, own, weight, pbuf, tokens, owf, total, res, normed, sgu, sdown,
    halo_send, halo_recv, p_send, p_recv, core_send, core_recv, far_send, far_recv,
    z_send, z_recv, o_send, o_recv, d_send, d_recv, l_sem,
):
    f32, bf16 = jnp.float32, jnp.bfloat16
    block = tokens.shape[1]
    quarters = tokens.shape[0]
    tok_local, group = own.shape
    width = out_weight.shape[1]
    half = group // 2
    pieces = far_send.shape[0]
    piece = width // pieces
    me = lax.axis_index("sp")
    tp = lax.axis_index("tp")
    count = 2 * length
    spot = me // 2
    tp_core = tp + 1 - 2 * (tp % 2)
    tp_far = (tp + quarters // 2) % quarters
    tp_other = tp + 3 - 2 * (tp % 2) - 2 * ((tp // 2) * 2)
    z_mate = me + 2 - 4 * (spot % 2)
    mate = me + 1 - 2 * (me % 2)
    inner = shared_gate.shape[1]
    part = wdp.shape[1]
    d_pieces = d_send.shape[1]
    d_piece = width // d_pieces
    early, far_early = d_pieces - 1, 1
    mine, theirs = spot % 2, 1 - spot % 2
    has_prev, has_next = me > 0, me < count - 1
    barrier = pltpu.get_barrier_semaphore()

    def greet(device):
        pl.semaphore_signal(barrier, inc=1, device_id=device, device_id_type=MESH)

    for peer in (tp_core, tp_far, tp_other):
        greet({"tp": peer})
    greet({"sp": z_mate})
    greet({"sp": mate})
    across = me + 2 * (me % 2) - 1
    has_across = (across >= 0) & (across < count)
    pl.when(has_across)(lambda: greet({"sp": across}))
    pl.semaphore_wait(barrier, 5 + has_across.astype(jnp.int32))

    def remote(src, dst, send, recv, device):
        return pltpu.make_async_remote_copy(
            src_ref=src, dst_ref=dst, send_sem=send, recv_sem=recv, device_id=device, device_id_type=MESH
        )

    def cut(side, i):
        return pl.ds(pl.multiple_of(side * half, half), half), pl.ds(i * piece, piece)

    def to_next():
        return remote(pool_in.at[pl.ds(tok_local - 16, 16)], halo.at[0], halo_send.at[0], halo_recv.at[0], {"sp": me + 1})

    def to_prev():
        return remote(pool_in.at[pl.ds(0, 16)], halo.at[1], halo_send.at[1], halo_recv.at[1], {"sp": me - 1})

    def far_copy(i):
        r, c = cut(mine, i)
        return remote(out_weight.at[r, c], owf.at[2, r, c], far_send.at[i], far_recv.at[i], {"tp": tp_far})

    def core_copy():
        return remote(out_weight, owf.at[1], core_send.at[0], core_recv.at[0], {"tp": tp_core})

    def z_copy(side, i):
        r, c = cut(side, i)
        return remote(owf.at[2, r, c], owf.at[2, r, c], z_send.at[i], z_recv.at[i], {"sp": z_mate})

    def other_copy(side, i):
        r, c = cut(side, i)
        return remote(owf.at[2, r, c], owf.at[3, r, c], o_send.at[side, i], o_recv.at[side, i], {"tp": tp_core})

    def block_copy(b):
        return remote(pbuf.at[b], tokens.at[tp], p_send.at[b], p_recv.at[tp], {"tp": b})

    def down_copy(slot, p):
        cols = pl.ds(p * d_piece, d_piece)
        src = down.at[pl.ds(pl.multiple_of(tp * part, 8), part), cols] if slot == 0 else wdp.at[2 if slot == 3 else 0, :, cols]
        device = ({"sp": mate}, {"tp": tp_core}, {"tp": tp_far}, {"tp": tp_core})[slot]
        return remote(src, wdp.at[slot, :, cols], d_send.at[slot, p], d_recv.at[slot, p], device)

    def down_arrived(p):
        down_copy(0, p).wait_recv()
        down_copy(1, p).start()
        if p < far_early:
            down_copy(2, p).start()

    def down_relayed(p):
        down_copy(2, p).wait_recv()
        down_copy(3, p).start()

    pl.when(has_next)(lambda: to_next().start())
    pl.when(has_prev)(lambda: to_prev().start())
    for i in range(pieces):
        far_copy(i).start()
    for p in range(early):
        down_copy(0, p).start()
    core_copy().start()
    loads = [
        pltpu.make_async_copy(pool_in, own, l_sem.at[0]),
        pltpu.make_async_copy(pool_weight.at[0], weight, l_sem.at[1]),
        pltpu.make_async_copy(out_weight, owf.at[0], l_sem.at[2]),
        pltpu.make_async_copy(resid, res, l_sem.at[3]),
        pltpu.make_async_copy(shared_gate, sgu.at[:, pl.ds(0, inner)], l_sem.at[4]),
        pltpu.make_async_copy(shared_up, sgu.at[:, pl.ds(inner, inner)], l_sem.at[5]),
        pltpu.make_async_copy(shared_down, sdown, l_sem.at[6]),
    ]
    for load in loads:
        load.start()

    zeros = jnp.zeros((16, group), f32)
    padded[0:16] = zeros
    padded[16 + tok_local : 32 + tok_local] = zeros
    loads[0].wait()
    loads[1].wait()
    padded[16 : 16 + tok_local] = own[...].astype(f32)

    @pl.when(has_prev)
    def _():
        to_next().wait_recv()
        padded[0:16] = halo[0].astype(f32)

    @pl.when(has_next)
    def _():
        to_prev().wait_recv()
        padded[16 + tok_local : 32 + tok_local] = halo[1].astype(f32)

    seq_total = tok_local * count
    for b in range(quarters):
        start = b * block
        positions = me * tok_local + start + lax.broadcasted_iota(jnp.int32, (block, group), 0)
        running = jnp.zeros((block, group), f32)
        chosen = running
        covered = 0
        for number in range(4):
            span = 2**number
            for shift in list(range(-span, -covered)) + list(range(covered, span)):
                running = running + padded[16 + start + shift : 16 + start + shift + block]
            covered = span
            held = jnp.minimum(positions + span, seq_total) - jnp.maximum(positions - span, 0)
            average = running / held.astype(f32)
            chosen = average if number == 0 else jnp.where(tp == number, average, chosen)
        spread = (chosen - padded[16 + start : 16 + start + block]).astype(bf16)
        mixed = jnp.dot(spread, weight[...], preferred_element_type=f32)
        pbuf[b] = (mixed * pool_scale[...]).astype(bf16)
        pl.when(tp != b)(lambda: block_copy(b).start())

        @pl.when(tp == b)
        def _():
            tokens[b] = pbuf[b]

    for i in range(pieces):
        far_copy(i).wait_recv()
        z_copy(mine, i).start()
        other_copy(mine, i).start()
        if i == 0:
            down_arrived(0)

    loads[2].wait()
    core_copy().wait_recv()
    loads[3].wait()

    def taken(peer):
        remote(pbuf.at[0], tokens.at[peer], p_send.at[0], p_recv.at[peer], {"tp": peer}).wait_recv()

    step = width // 4

    def add(slots, first):
        def one(q, carry):
            cols = pl.ds(pl.multiple_of(q * step, step), step)
            value = res[:, cols].astype(f32) if first else total[:, cols]
            branch = jnp.zeros_like(value) if first else value
            for slot, peer in slots:
                branch = branch + jnp.dot(tokens[peer], owf[slot, :, cols], preferred_element_type=f32)
            total[:, cols] = branch
            return carry

        lax.fori_loop(0, width // step, one, 0)

    taken(tp_core)
    add(((0, tp), (1, tp_core)), True)
    taken(tp_far)
    taken(tp_other)
    for i in range(pieces):
        z_copy(theirs, i).wait_recv()
        other_copy(theirs, i).start()
    for i in range(pieces):
        other_copy(mine, i).wait_recv()
        other_copy(theirs, i).wait_recv()
    down_arrived(1)
    add(((2, tp_far), (3, tp_other)), False)

    def square(q, carry):
        cols = pl.ds(pl.multiple_of(q * step, step), step)
        mid = (res[:, cols].astype(f32) + total[:, cols]).astype(bf16)
        res[:, cols] = mid
        wide = mid.astype(f32)
        return carry + jnp.sum(wide * wide, axis=1, keepdims=True)

    sums = lax.fori_loop(0, width // step, square, jnp.zeros((block, 1), f32))
    scale = lax.rsqrt(sums / width + norm_eps)

    def spread_norm(q, carry):
        cols = pl.ds(pl.multiple_of(q * step, step), step)
        normed[:, cols] = (res[:, cols].astype(f32) * scale * gain[:, cols]).astype(bf16)
        return carry

    lax.fori_loop(0, width // step, spread_norm, 0)
    put_normed = pltpu.make_async_copy(normed, normed_out, l_sem.at[0])
    put_normed.start()
    for load in loads[4:]:
        load.wait()
    both = jnp.dot(normed[...], sgu[...], preferred_element_type=f32)
    hidden = (jax.nn.silu(both[:, :inner]) * both[:, inner:]).astype(bf16)

    def shared(q, carry):
        cols = pl.ds(pl.multiple_of(q * step, step), step)
        total[:, cols] = res[:, cols].astype(f32) + jnp.dot(hidden, sdown[:, cols], preferred_element_type=f32)
        return carry

    lax.fori_loop(0, width // step, shared, 0)
    put_base = pltpu.make_async_copy(total, base, l_sem.at[1])
    put_base.start()
    down_relayed(0)
    down_arrived(2)
    for p in range(early):
        down_copy(1, p).wait_recv()
        if p < far_early:
            down_copy(3, p).wait_recv()
            down_copy(2, p).wait_send()
            down_copy(3, p).wait_send()
        down_copy(0, p).wait_send()
        down_copy(1, p).wait_send()
    put_normed.wait()
    put_base.wait()

    pl.when(has_next)(lambda: to_next().wait_send())
    pl.when(has_prev)(lambda: to_prev().wait_send())
    core_copy().wait_send()
    for i in range(pieces):
        far_copy(i).wait_send()
        z_copy(mine, i).wait_send()
        other_copy(mine, i).wait_send()
        other_copy(theirs, i).wait_send()
    for b in range(quarters):
        pl.when(tp != b)(lambda: block_copy(b).wait_send())


def mixer(pool_in, pool_weight, pool_scale, out_weight, resid, gain, shared_gate, shared_up, shared_down, down):
    count = lax.axis_size("sp")
    quarters = lax.axis_size("tp")
    length = count // 2
    tok_local, group = pool_in.shape
    assert pool_weight.shape[0] == 1 and quarters == 4 and length % 2 == 0
    rows, width = resid.shape
    bf16, f32 = jnp.bfloat16, jnp.float32
    dma = pltpu.SemaphoreType.DMA
    pieces = 2
    deep = down.shape[0]
    inner = shared_gate.shape[1]
    anywhere = pl.BlockSpec(memory_space=pl.ANY)
    local = pl.BlockSpec(memory_space=pltpu.VMEM)
    return pl.pallas_call(
        functools.partial(mixer_kernel, length),
        out_shape=[
            jax.ShapeDtypeStruct((rows, width), f32),
            jax.ShapeDtypeStruct((rows, width), bf16),
            jax.ShapeDtypeStruct((quarters, deep // quarters, width), bf16),
        ],
        in_specs=[anywhere, anywhere, local, anywhere, anywhere, local] + [anywhere] * 4,
        out_specs=[anywhere] * 3,
        scratch_shapes=[
            pltpu.VMEM((tok_local + 32, group), f32),
            pltpu.VMEM((2, 16, group), bf16),
            pltpu.VMEM((tok_local, group), bf16),
            pltpu.VMEM((group, group), bf16),
            pltpu.VMEM((quarters, rows, group), bf16),
            pltpu.VMEM((quarters, rows, group), bf16),
            pltpu.VMEM((quarters, group, width), bf16),
            pltpu.VMEM((rows, width), f32),
            pltpu.VMEM((rows, width), bf16),
            pltpu.VMEM((rows, width), bf16),
            pltpu.VMEM((width, 2 * inner), bf16),
            pltpu.VMEM((inner, width), bf16),
            dma((2,)), dma((2,)), dma((quarters,)), dma((quarters,)), dma((1,)), dma((1,)),
            dma((pieces,)), dma((pieces,)), dma((pieces,)), dma((pieces,)),
            dma((2, pieces)), dma((2, pieces)), dma((4, 4)), dma((4, 4)), dma((7,)),
        ],
        compiler_params=pltpu.CompilerParams(
            collective_id=1, has_side_effects=True, vmem_limit_bytes=56 * 2**20
        ),
        cost_estimate=pl.CostEstimate(flops=10**11, bytes_accessed=10**8, transcendentals=0),
    )(
        pool_in, pool_weight, pool_scale[None, :], out_weight, resid, gain[None, :],
        shared_gate, shared_up, shared_down, down,
    )


def moe_kernel(
    length, cap, quarters,
    x, mt, wdp_in, gate, up, down, base,
    out, wdp, inbuf,
    xbuf, mbuf, wgu, wdbuf, xr, xp, ho, hsp, hits, hacc, hp, hr, m8, stage, total_out, out_stage,
    x_send, x_recv, m_send, m_recv, y_send, y_recv, h_send, h_recv, r_send, r_recv,
    wd_send, wd_recv, w_sem, s_sem, l_sem, own_sem,
):
    f32, bf16 = jnp.float32, jnp.bfloat16
    rows, width = x.shape
    local, _, inner = gate.shape
    deep = local * inner
    total = local * 2 * length
    rows_y = xr.shape[0]
    pieces = r_send.shape[1]
    piece = width // pieces
    chunk = wdbuf.shape[2]
    chunks = width // chunk
    part = wdp.shape[1]
    me = lax.axis_index("sp")
    tp = lax.axis_index("tp")
    spot, side = me // 2, me % 2
    mate = me + 1 - 2 * side
    tp_core = tp + 1 - 2 * (tp % 2)
    tp_far = (tp + quarters // 2) % quarters
    last = length - 1
    has_left, has_right = spot > 0, spot < last
    barrier = pltpu.get_barrier_semaphore()

    def greet(device):
        pl.semaphore_signal(barrier, inc=1, device_id=device, device_id_type=MESH)

    greet({"sp": mate})
    greet({"tp": tp_core})
    greet({"tp": tp_far})

    @pl.when(has_left)
    def _():
        greet({"sp": me - 2})

    @pl.when(has_right)
    def _():
        greet({"sp": me + 2})

    pl.semaphore_wait(barrier, 3 + jnp.minimum(spot, 1) + jnp.minimum(last - spot, 1))

    def remote(src, dst, send, recv, device):
        return pltpu.make_async_remote_copy(
            src_ref=src, dst_ref=dst, send_sem=send, recv_sem=recv, device_id=device, device_id_type=MESH
        )

    def cols_of(q):
        return pl.ds(pl.multiple_of(q * piece, piece), piece)

    def onward(way):
        return {"sp": me + 2} if way == 0 else {"sp": me - 2}

    def row_copy(way, source, q, src):
        cols = cols_of(q)
        return remote(
            src.at[:, cols], xbuf.at[source, :, cols], x_send.at[way, source, q], x_recv.at[source, q], onward(way)
        )

    def table_copy(way, source, src):
        return remote(src, mbuf.at[source], m_send.at[way, source], m_recv.at[source], onward(way))

    def each_piece(act):
        def one(q, carry):
            act(q)
            return carry

        lax.fori_loop(0, pieces, one, 0)

    def send_own(way):
        table_copy(way, spot, mt).start()
        each_piece(lambda q: row_copy(way, spot, q, x).start())

    pl.when(has_right)(lambda: send_own(0))
    pl.when(has_left)(lambda: send_own(1))

    own_rows = pltpu.make_async_copy(x, xbuf.at[spot], own_sem.at[0])
    own_table = pltpu.make_async_copy(mt, mbuf.at[spot], own_sem.at[1])
    own_rows.start()
    own_table.start()

    d_pieces = wd_send.shape[1]
    d_piece = width // d_pieces
    end_piece = d_pieces - 1

    def quarter_copy(slot, p):
        cols = pl.ds(p * d_piece, d_piece)
        if slot == 0:
            src = down.at[pl.ds(pl.multiple_of(tp * part, 8), part), cols]
        else:
            src = wdp.at[2 if slot == 3 else 0, :, cols]
        device = ({"sp": mate}, {"tp": tp_core}, {"tp": tp_far}, {"tp": tp_core})[slot]
        return remote(src, wdp.at[slot, :, cols], wd_send.at[slot, p], wd_recv.at[slot, p], device)

    gate_load = pltpu.make_async_copy(gate, wgu.at[:, :, pl.ds(0, inner)], w_sem.at[0])
    up_load = pltpu.make_async_copy(up, wgu.at[:, :, pl.ds(inner, inner)], w_sem.at[1])
    gate_load.start()
    up_load.start()
    quarter_copy(0, end_piece).start()
    for p in range(1, end_piece):
        quarter_copy(2, p).start()
    base_load = pltpu.make_async_copy(base, total_out, own_sem.at[2])
    base_load.start()

    def source_of(j):
        close = jnp.minimum(spot, last - spot)
        near = jnp.where(j % 2 == 1, spot - (j + 1) // 2, spot + j // 2)
        far = jnp.where(spot < last - spot, spot + j - close, spot - (j - close))
        return jnp.where(j <= 2 * close, near, far)

    def take_piece(hop, q):
        def take(source, way, goes_on):
            row_copy(way, source, q, xbuf.at[source]).wait_recv()
            pl.when(goes_on)(lambda: row_copy(way, source, q, xbuf.at[source]).start())

            @pl.when(q == 0)
            def _():
                table_copy(way, source, mbuf.at[source]).wait_recv()
                pl.when(goes_on)(lambda: table_copy(way, source, mbuf.at[source]).start())

        pl.when(spot >= hop)(lambda: take(spot - hop, 0, has_right))
        pl.when(spot + hop <= last)(lambda: take(spot + hop, 1, has_left))

    def slot_hits(table, e):
        place = table[:, 5 * local + e : 5 * local + e + 1]
        columns = lax.broadcasted_iota(jnp.int32, (rows, rows_y), 1).astype(f32)
        return ((place >= 0.0) & (columns == place + float(cap * e))).astype(f32)

    def weight_of(table, i):
        return table[:, i : i + 1] + table[:, 2 * local + i : 2 * local + i + 1]

    def y_copy(j, q):
        cols = cols_of(q)
        return remote(xr.at[:, cols], xp.at[j % 2, :, cols], y_send.at[q], y_recv.at[j % 2, q], {"sp": mate})

    def h_copy(j):
        return remote(hp, hr.at[j], h_send.at[0], h_recv.at[j], {"sp": mate})

    def keep_table(j):
        c = lax.broadcasted_iota(jnp.int32, (128, 128), 1)
        group = (c >= 2 * local).astype(jnp.int32) + (c >= 4 * local).astype(jnp.int32)
        i = c - 2 * local * group
        expert = jnp.where(i < local, me * local + i, mate * local + i - local)
        choose = (lax.broadcasted_iota(jnp.int32, (128, 128), 0) == group * total + expert) & (c < 6 * local)
        m8[j] = jnp.dot(mbuf[source_of(j)], choose.astype(f32).astype(bf16), preferred_element_type=f32)

    def gather_piece(j, q):
        source = source_of(j)

        @pl.when(q == 0)
        def _():
            pl.when(j > 0)(lambda: keep_table(j))
            table = m8[j]
            found = slot_hits(table, 0)
            for e in range(1, local):
                found = found + slot_hits(table, e)
            hits[...] = found.astype(bf16)

        pl.when(j != 1)(lambda: y_copy(j, q).wait_send())
        cols = cols_of(q)
        xr[:, cols] = lax.dot_general(
            hits[...], xbuf[source, :, cols], (((0,), (0,)), ((), ())), preferred_element_type=f32
        ).astype(bf16)
        y_copy(j, q).start()

    def gated(lhs, e):
        both = jnp.dot(lhs, wgu[e], preferred_element_type=f32)
        return jax.nn.silu(both[:, :inner]) * both[:, inner:]

    def own_hidden(j, first, end):
        source = source_of(j)

        def one(e, carry):
            table = m8[j]
            lanes = lax.broadcasted_iota(jnp.int32, table.shape, 1)
            mine = jnp.where((lanes == e) | (lanes == 2 * local + e), table, 0.0)
            weight = jnp.sum(mine, axis=1, keepdims=True)
            cols = pl.ds(pl.multiple_of(e * inner, 128), inner)
            ho[jnp.minimum(j, 1), :, cols] = (gated(xbuf[source], e) * weight).astype(bf16)
            return carry

        lax.fori_loop(first, end, one, 0)

    cover = max(-(-(cap * (e + 1)) // 16) * 16 - cap * e // 16 * 16 for e in range(local))

    def mate_hidden(j):
        each_piece(lambda q: y_copy(j, q).wait_recv())
        hacc[...] = jnp.zeros_like(hacc)

        def one(e, carry):
            first = pl.multiple_of(cap * e // 16 * 16, 16)
            found = gated(xp[j % 2, pl.ds(first, cover), :], e)
            spots = lax.broadcasted_iota(jnp.int32, found.shape, 0) + first
            keep = (spots >= cap * e) & (spots < cap * (e + 1))
            hacc[pl.ds(first, cover), :] += jnp.where(keep, found, 0.0)
            return carry

        lax.fori_loop(0, local, one, 0)

        pl.when(j != 1)(lambda: h_copy(j).wait_send())
        hp[...] = hacc[...].astype(bf16)
        h_copy(j).start()

    def down_copies(c, slot):
        cols = pl.ds(pl.multiple_of(c * chunk, chunk), chunk)
        copies = [pltpu.make_async_copy(down.at[:, cols], wdbuf.at[slot, pl.ds(0, deep), :], s_sem.at[slot, 0])]
        where = (tp, tp_core, tp_far, tp + 3 - 2 * (tp % 2) - 2 * ((tp // 2) * 2))
        for n in range(quarters):
            src = wdp.at[n, :, cols]
            place = pl.ds(pl.multiple_of(deep + where[n] * part, 16), part)
            copies.append(pltpu.make_async_copy(src, wdbuf.at[slot, place, :], s_sem.at[slot, 1 + n]))
        return copies

    def load_down(c, slot):
        for copy in down_copies(c, slot):
            copy.start()

    def return_copy(way, source, q):
        cols = cols_of(q)
        target = jnp.where(spot + 1 == source, length, source) if way == 0 else source
        return remote(
            xbuf.at[source, :, cols], inbuf.at[target, :, cols], r_send.at[source, q], r_recv.at[target, q], onward(way)
        )

    def return_wait(slot, q):
        cols = cols_of(q)
        remote(
            xbuf.at[0, :, cols], inbuf.at[slot, :, cols], r_send.at[0, q], r_recv.at[slot, q], {"sp": mate}
        ).wait_recv()

    def scatter_hidden(j):
        table = m8[j]
        for e in range(local):
            spread = jnp.dot(slot_hits(table, e).astype(bf16), hr[j], preferred_element_type=f32)
            hsp[:, e * inner : (e + 1) * inner] = (spread * weight_of(table, local + e)).astype(bf16)

    ratio = chunks // pieces

    def down_chunk(j, c):
        slot = c % 2
        pl.when(c + 1 < chunks)(lambda: load_down(c + 1, 1 - slot))
        for copy in down_copies(c, slot):
            copy.wait()
        cols = pl.ds(pl.multiple_of(c * chunk, chunk), chunk)
        result = jnp.dot(ho[jnp.minimum(j, 1)], wdbuf[slot, :deep, :], preferred_element_type=f32)
        return cols, result + jnp.dot(hsp[...], wdbuf[slot, deep:, :], preferred_element_type=f32)

    def project(j, first, end):
        source = source_of(j)

        def one(c, carry):
            fresh = c % ratio == 0
            pl.when(fresh & (source < spot) & has_right)(
                lambda: row_copy(0, source, c // ratio, xbuf.at[source]).wait_send()
            )
            pl.when(fresh & (source > spot) & has_left)(
                lambda: row_copy(1, source, c // ratio, xbuf.at[source]).wait_send()
            )
            cols, result = down_chunk(j, c)
            xbuf[source, :, cols] = result.astype(bf16)
            whole = c % ratio == ratio - 1

            @pl.when(whole & (spot == last) & (source < spot))
            def _():
                return_copy(1, source, c // ratio).start()

            @pl.when(whole & (spot == 0) & (source > spot))
            def _():
                return_copy(0, source, c // ratio).start()

            return carry

        lax.fori_loop(first, end, one, 0)

    def project_own(first, end):
        def one(c, carry):
            cols, result = down_chunk(0, c)
            total_out[:, cols] += result
            return carry

        lax.fori_loop(first, end, one, 0)

    def fold(slot, q, n):
        cols = cols_of(q)
        if stage is None:
            return inbuf[slot, :, cols].astype(f32)
        copy = pltpu.make_async_copy(inbuf.at[slot, :, cols], stage.at[n], l_sem.at[n])
        copy.start()
        copy.wait()
        return stage[n].astype(f32)

    def relay(k, first, end):
        def hand_on(way, source, q):
            cols = cols_of(q)
            return_wait(source, q)
            both = xbuf[source, :, cols].astype(f32) + fold(source, q, way)
            xbuf[source, :, cols] = both.astype(bf16)
            return_copy(way, source, q).start()

        def one(tau, carry):
            left, right = tau - (last - spot), tau - spot

            @pl.when((spot > last - k) & has_right & (left >= 0) & (left < pieces))
            def _():
                hand_on(1, last - k, left)

            @pl.when((spot < k) & has_left & (right >= 0) & (right < pieces))
            def _():
                hand_on(0, k, right)

            return carry

        lax.fori_loop(first, end, one, 0)

    middle = chunks // 2

    def window(w, carry):
        j = w - 1
        pl.when(w >= 4)(lambda: relay(w - 2, 1, 2))
        pl.when(w >= 2)(lambda: own_hidden(j, 0, local))
        pl.when(w >= 4)(lambda: relay(w - 2, 2, 3))

        def one(q, inner_carry):
            @pl.when(w < length)
            def _():
                take_piece(w, q)
                gather_piece(w, q)

            @pl.when((w == 1) & (q == 0))
            def _():
                gate_load.wait()
                up_load.wait()
                own_hidden(0, 0, local)
                quarter_copy(0, end_piece).wait_recv()
                quarter_copy(1, end_piece).start()
                quarter_copy(2, end_piece).start()

            @pl.when((w == 1) & (q == 3))
            def _():
                for p in range(1, end_piece):
                    quarter_copy(2, p).wait_recv()
                    quarter_copy(3, p).start()

            @pl.when((w >= 2) & (q == 0))
            def _():
                mate_hidden(j)
                pl.when(w > 2)(lambda: load_down(0, 0))
                pl.when(w >= 4)(lambda: relay(w - 2, 3, 4))

            @pl.when((w >= 2) & (q == 1))
            def _():
                @pl.when(w == 2)
                def _():
                    quarter_copy(2, end_piece).wait_recv()
                    quarter_copy(3, end_piece).start()
                    quarter_copy(1, end_piece).wait_recv()
                    for p in range(1, d_pieces):
                        quarter_copy(3, p).wait_recv()
                    load_down(0, 0)

                h_copy(j).wait_recv()
                scatter_hidden(j)

            @pl.when((w >= 2) & ((q == 1) | (q == 2)))
            def _():
                project(j, (q - 1) * middle, q * middle)

            pl.when((w >= 4) & (q == 1))(lambda: relay(w - 2, 4, pieces + last))
            pl.when((w == length) & (q == 1))(lambda: each_piece(lambda p: gather_piece(0, p)))
            return inner_carry

        return lax.fori_loop(0, pieces, one, carry)

    own_rows.wait()
    own_table.wait()
    keep_table(0)
    lax.fori_loop(1, length + 1, window, 0)
    relay(last, 1, 4)
    mate_hidden(0)
    load_down(0, 0)
    relay(last, 4, 5)
    h_copy(0).wait_recv()
    scatter_hidden(0)
    base_load.wait()
    project_own(0, middle)
    relay(last, 5, pieces + last)
    project_own(middle, chunks)

    def out_copy(q):
        cols = cols_of(q)
        return pltpu.make_async_copy(out_stage.at[:, cols], out.at[:, cols], s_sem.at[0, q])

    def finish(q, carry):
        cols = cols_of(q)

        @pl.when(has_right)
        def _():
            return_wait(spot, q)
            total_out[:, cols] += fold(spot, q, 0)

        @pl.when(has_left)
        def _():
            return_wait(length, q)
            total_out[:, cols] += fold(length, q, 1)

        out_stage[:, cols] = total_out[:, cols].astype(bf16)
        out_copy(q).start()
        return carry

    lax.fori_loop(0, pieces, finish, 0)
    each_piece(lambda q: out_copy(q).wait())

    each_piece(lambda q: y_copy(0, q).wait_send())
    h_copy(0).wait_send()
    for slot in (0, 1):
        quarter_copy(slot, end_piece).wait_send()
    for p in range(1, d_pieces):
        quarter_copy(2, p).wait_send()
        quarter_copy(3, p).wait_send()

    def drain_own(way):
        each_piece(lambda q: row_copy(way, spot, q, x).wait_send())

    pl.when(has_right)(lambda: drain_own(0))
    pl.when(has_left)(lambda: drain_own(1))

    def drain(s, carry):
        pl.when((s <= spot) & has_right)(lambda: table_copy(0, s, mbuf.at[s]).wait_send())
        pl.when((s >= spot) & has_left)(lambda: table_copy(1, s, mbuf.at[s]).wait_send())

        @pl.when(s != spot)
        def _():
            each_piece(lambda q: return_copy(1, s, q).wait_send())

        return carry

    lax.fori_loop(0, length, drain, 0)


def routed_experts(normed, route_ids, route_weight, expert_gate, expert_up, expert_down, mate_down, base):
    count = lax.axis_size("sp")
    quarters = lax.axis_size("tp")
    assert count % 2 == 0 and count >= 6 and quarters == 4
    length = count // 2
    local, _, inner = expert_gate.shape
    total = local * count
    rows, width = normed.shape
    pieces = 4
    piece = width // pieces
    chunk = piece // 2
    cap = expert_slots
    rows_y = -(-(cap * local) // 16) * 16
    table, coarse, fine, place = routing_table(route_ids, route_weight, total)
    pad = 128 - 3 * total
    mt = jnp.concatenate([coarse, fine, place, jnp.zeros((rows, pad), jnp.bfloat16)], axis=1)
    deep = local * inner
    bf16, f32 = jnp.bfloat16, jnp.float32
    dma = pltpu.SemaphoreType.DMA
    anywhere = pl.BlockSpec(memory_space=pl.ANY)
    landing = (length + 1, rows, width)
    direct = 2 * math.prod(landing) < 12 * 2**20
    scratch = [
        pltpu.VMEM((length, rows, width), bf16),
        pltpu.VMEM((length, rows, 128), bf16),
        pltpu.VMEM((local, width, 2 * inner), bf16),
        pltpu.VMEM((2, 2 * deep, chunk), bf16),
        pltpu.VMEM((rows_y, width), bf16),
        pltpu.VMEM((2, rows_y, width), bf16),
        pltpu.VMEM((2, rows, deep), bf16),
        pltpu.VMEM((rows, deep), bf16),
        pltpu.VMEM((rows, rows_y), bf16),
        pltpu.VMEM((rows_y, inner), f32),
        pltpu.VMEM((rows_y, inner), bf16),
        pltpu.VMEM((length, rows_y, inner), bf16),
        pltpu.VMEM((length, rows, 128), f32),
        None if direct else pltpu.VMEM((2, rows, piece), bf16),
        pltpu.VMEM((rows, width), f32),
        pltpu.VMEM((rows, width), bf16),
        dma((2, length, pieces)), dma((length, pieces)), dma((2, length)), dma((length,)),
        dma((pieces,)), dma((2, pieces)), dma((1,)), dma((length,)),
        dma((length, pieces)), dma((length + 1, pieces)),
        dma((4, 4)), dma((4, 4)), dma((2,)), dma((2, 1 + quarters)), dma((2,)), dma((3,)),
    ]
    outs = [
        jax.ShapeDtypeStruct((rows, width), bf16),
        jax.ShapeDtypeStruct((quarters, deep // quarters, width), bf16),
    ]
    kernel = functools.partial(moe_kernel, length, cap, quarters)
    if direct:
        scratch.insert(0, pltpu.VMEM(landing, bf16))
        gap = 9 + 1 + 13
        scratch.remove(None)

        def body(*refs):
            return kernel(*refs[:gap], None, *refs[gap:])
    else:
        outs.append(jax.ShapeDtypeStruct(landing, bf16))
        body = kernel
    results = pl.pallas_call(
        body,
        out_shape=outs,
        in_specs=[anywhere] * 7,
        out_specs=[anywhere] * len(outs),
        input_output_aliases={2: 1},
        scratch_shapes=scratch,
        compiler_params=pltpu.CompilerParams(
            collective_id=0, has_side_effects=True, vmem_limit_bytes=67043328
        ),
    )(normed, mt, mate_down, expert_gate, expert_up, expert_down.reshape(deep, width), base)
    return results[0]


def routing_table(route_ids, route_weight, total):
    rows = route_ids.shape[0]
    names = lax.iota(jnp.int32, total)
    named = route_ids[:, :, None] == names[None, None, :]
    table = jnp.sum(jnp.where(named, route_weight[:, :, None], 0.0), axis=1)
    member = jnp.any(named, axis=1)
    before = (lax.iota(jnp.int32, rows)[:, None] > lax.iota(jnp.int32, rows)[None, :]).astype(jnp.bfloat16)
    rank = jnp.dot(before, member.astype(jnp.bfloat16), preferred_element_type=jnp.float32)
    place = jnp.where(member, rank, -1.0).astype(jnp.bfloat16)
    coarse = table.astype(jnp.bfloat16)
    fine = (table - coarse.astype(jnp.float32)).astype(jnp.bfloat16)
    return table, coarse, fine, place


def shards(
    resid,
    pool_in,
    pool_weight,
    pool_scale,
    out_weight,
    norm_gain,
    route_ids,
    route_weight,
    expert_gate,
    expert_up,
    expert_down,
    shared_gate,
    shared_up,
    shared_down,
):
    flat_down = expert_down.reshape(-1, expert_down.shape[2])
    base, normed, mate_down = mixer(
        pool_in, pool_weight, pool_scale, out_weight, resid, norm_gain, shared_gate, shared_up, shared_down, flat_down
    )
    return routed_experts(
        normed, route_ids, route_weight, expert_gate, expert_up, expert_down, mate_down, base
    )


def solution(mesh):
    return jax.shard_map(
        shards,
        mesh=mesh,
        in_specs=(
            P(("sp", "tp"), None),
            P("sp", "tp"),
            P("tp", None, None),
            P("tp"),
            P("tp", None),
            P(),
            P(("sp", "tp"), None),
            P(("sp", "tp"), None),
            P("sp", None, None),
            P("sp", None, None),
            P("sp", None, None),
            P(),
            P(),
            P(),
        ),
        out_specs=P(("sp", "tp"), None),
        check_vma=False,
    )
```

```python
import functools
import math

import jax
import jax.numpy as jnp
from jax import lax
from jax.experimental import pallas as pl
from jax.experimental.pallas import tpu as pltpu
from jax.sharding import PartitionSpec as P

norm_eps = 1e-06
expert_slots = 36
MESH = pl.DeviceIdType.MESH


def mixer_kernel(
    length, experts, pool_in, pool_weight, pool_scale, out_weight, resid, gain, shared_gate, shared_up, shared_down, down,
    ids, shares,
    base, normed_out, wdp, lead, mt,
    padded, halo, own, weight, pbuf, tokens, owf, total, res, normed, sgu, sdown,
    halo_send, halo_recv, p_send, p_recv, core_send, core_recv, far_send, far_recv,
    z_send, z_recv, o_send, o_recv, d_send, d_recv, lead_send, lead_recv, l_sem,
):
    f32, bf16 = jnp.float32, jnp.bfloat16
    block = tokens.shape[1]
    quarters = tokens.shape[0]
    tok_local, group = own.shape
    width = out_weight.shape[1]
    half = group // 2
    pieces = far_send.shape[0]
    piece = width // pieces
    me = lax.axis_index("sp")
    tp = lax.axis_index("tp")
    count = 2 * length
    spot = me // 2
    tp_core = tp + 1 - 2 * (tp % 2)
    tp_far = (tp + quarters // 2) % quarters
    tp_other = tp + 3 - 2 * (tp % 2) - 2 * ((tp // 2) * 2)
    z_mate = me + 2 - 4 * (spot % 2)
    mate = me + 1 - 2 * (me % 2)
    inner = shared_gate.shape[1]
    part = wdp.shape[1]
    d_pieces = d_send.shape[1]
    d_piece = width // d_pieces
    early, far_early = d_pieces - 1, 1
    mine, theirs = spot % 2, 1 - spot % 2
    has_prev, has_next = me > 0, me < count - 1
    barrier = pltpu.get_barrier_semaphore()

    def greet(device):
        pl.semaphore_signal(barrier, inc=1, device_id=device, device_id_type=MESH)

    for peer in (tp_core, tp_far, tp_other):
        greet({"tp": peer})
    greet({"sp": z_mate})
    greet({"sp": mate})
    across = me + 2 * (me % 2) - 1
    has_across = (across >= 0) & (across < count)
    z_next = me - 2 + 4 * (spot % 2)
    has_z_next = (z_next >= 0) & (z_next < count)
    pl.when(has_across)(lambda: greet({"sp": across}))
    pl.when(has_z_next)(lambda: greet({"sp": z_next}))
    pl.semaphore_wait(barrier, 5 + has_across.astype(jnp.int32) + has_z_next.astype(jnp.int32))

    def remote(src, dst, send, recv, device):
        return pltpu.make_async_remote_copy(
            src_ref=src, dst_ref=dst, send_sem=send, recv_sem=recv, device_id=device, device_id_type=MESH
        )

    def cut(side, i):
        return pl.ds(pl.multiple_of(side * half, half), half), pl.ds(i * piece, piece)

    def to_next():
        return remote(pool_in.at[pl.ds(tok_local - 16, 16)], halo.at[0], halo_send.at[0], halo_recv.at[0], {"sp": me + 1})

    def to_prev():
        return remote(pool_in.at[pl.ds(0, 16)], halo.at[1], halo_send.at[1], halo_recv.at[1], {"sp": me - 1})

    def far_copy(i):
        r, c = cut(mine, i)
        return remote(out_weight.at[r, c], owf.at[2, r, c], far_send.at[i], far_recv.at[i], {"tp": tp_far})

    def core_copy():
        return remote(out_weight, owf.at[1], core_send.at[0], core_recv.at[0], {"tp": tp_core})

    def z_copy(side, i):
        r, c = cut(side, i)
        return remote(owf.at[2, r, c], owf.at[2, r, c], z_send.at[i], z_recv.at[i], {"sp": z_mate})

    def other_copy(side, i):
        r, c = cut(side, i)
        return remote(owf.at[2, r, c], owf.at[3, r, c], o_send.at[side, i], o_recv.at[side, i], {"tp": tp_core})

    def block_copy(b):
        return remote(pbuf.at[b], tokens.at[tp], p_send.at[b], p_recv.at[tp], {"tp": b})

    def down_copy(slot, p):
        cols = pl.ds(p * d_piece, d_piece)
        src = down.at[pl.ds(pl.multiple_of(tp * part, 8), part), cols] if slot == 0 else wdp.at[2 if slot == 3 else 0, :, cols]
        device = ({"sp": mate}, {"tp": tp_core}, {"tp": tp_far}, {"tp": tp_core})[slot]
        return remote(src, wdp.at[slot, :, cols], d_send.at[slot, p], d_recv.at[slot, p], device)

    has_left, has_right = spot > 0, spot < length - 1

    def lead_copy(way):
        device = {"sp": me + 2} if way == 0 else {"sp": me - 2}
        return remote(
            normed.at[:, pl.ds(0, lead.shape[2])], lead.at[way], lead_send.at[way], lead_recv.at[way], device
        )

    def down_arrived(p):
        down_copy(0, p).wait_recv()
        down_copy(1, p).start()
        if p < far_early:
            down_copy(2, p).start()

    def down_relayed(p):
        down_copy(2, p).wait_recv()
        down_copy(3, p).start()

    pl.when(has_next)(lambda: to_next().start())
    pl.when(has_prev)(lambda: to_prev().start())
    for i in range(pieces):
        far_copy(i).start()
    for p in range(early):
        down_copy(0, p).start()
    core_copy().start()
    loads = [
        pltpu.make_async_copy(pool_in, own, l_sem.at[0]),
        pltpu.make_async_copy(pool_weight.at[0], weight, l_sem.at[1]),
        pltpu.make_async_copy(out_weight, owf.at[0], l_sem.at[2]),
        pltpu.make_async_copy(resid, res, l_sem.at[3]),
        pltpu.make_async_copy(shared_gate, sgu.at[:, pl.ds(0, inner)], l_sem.at[4]),
        pltpu.make_async_copy(shared_up, sgu.at[:, pl.ds(inner, inner)], l_sem.at[5]),
        pltpu.make_async_copy(shared_down, sdown, l_sem.at[6]),
    ]
    for load in loads:
        load.start()

    zeros = jnp.zeros((16, group), f32)
    padded[0:16] = zeros
    padded[16 + tok_local : 32 + tok_local] = zeros
    loads[0].wait()
    loads[1].wait()
    padded[16 : 16 + tok_local] = own[...].astype(f32)

    @pl.when(has_prev)
    def _():
        to_next().wait_recv()
        padded[0:16] = halo[0].astype(f32)

    @pl.when(has_next)
    def _():
        to_prev().wait_recv()
        padded[16 + tok_local : 32 + tok_local] = halo[1].astype(f32)

    seq_total = tok_local * count
    for b in range(quarters):
        start = b * block
        positions = me * tok_local + start + lax.broadcasted_iota(jnp.int32, (block, group), 0)
        running = jnp.zeros((block, group), f32)
        chosen = running
        covered = 0
        for number in range(4):
            span = 2**number
            for shift in list(range(-span, -covered)) + list(range(covered, span)):
                running = running + padded[16 + start + shift : 16 + start + shift + block]
            covered = span
            held = jnp.minimum(positions + span, seq_total) - jnp.maximum(positions - span, 0)
            average = running / held.astype(f32)
            chosen = average if number == 0 else jnp.where(tp == number, average, chosen)
        spread = (chosen - padded[16 + start : 16 + start + block]).astype(bf16)
        mixed = jnp.dot(spread, weight[...], preferred_element_type=f32)
        pbuf[b] = (mixed * pool_scale[...]).astype(bf16)
        pl.when(tp != b)(lambda: block_copy(b).start())

        @pl.when(tp == b)
        def _():
            tokens[b] = pbuf[b]

    line = lax.broadcasted_iota(jnp.int32, (128, block), 0)
    kind = (line >= experts).astype(jnp.int32) + (line >= 2 * experts).astype(jnp.int32)
    expert = line - experts * kind
    share = jnp.zeros((128, block), f32)
    member = jnp.zeros((128, block), f32)
    for k in range(ids.shape[0]):
        hit = ids[k : k + 1, :] == expert
        share = share + jnp.where(hit, shares[k : k + 1, :], 0.0)
        member = member + jnp.where(hit, 1.0, 0.0)
    before = lax.broadcasted_iota(jnp.int32, (block, block), 0) < lax.broadcasted_iota(jnp.int32, (block, block), 1)
    rank = jnp.dot(member.astype(bf16), before.astype(f32).astype(bf16), preferred_element_type=f32)
    coarse = share.astype(bf16).astype(f32)
    entry = jnp.where(kind == 0, coarse, jnp.where(kind == 1, share - coarse, jnp.where(member > 0.0, rank, -1.0)))
    mt[...] = jnp.transpose(jnp.where(line < 3 * experts, entry, 0.0)).astype(bf16)

    for i in range(pieces):
        far_copy(i).wait_recv()
        z_copy(mine, i).start()
        other_copy(mine, i).start()
        if i == 0:
            down_arrived(0)

    loads[2].wait()
    core_copy().wait_recv()
    loads[3].wait()

    def taken(peer):
        remote(pbuf.at[0], tokens.at[peer], p_send.at[0], p_recv.at[peer], {"tp": peer}).wait_recv()

    step = width // 4

    def add(slots, first):
        def one(q, carry):
            cols = pl.ds(pl.multiple_of(q * step, step), step)
            value = res[:, cols].astype(f32) if first else total[:, cols]
            branch = jnp.zeros_like(value) if first else value
            for slot, peer in slots:
                branch = branch + jnp.dot(tokens[peer], owf[slot, :, cols], preferred_element_type=f32)
            total[:, cols] = branch
            return carry

        lax.fori_loop(0, width // step, one, 0)

    taken(tp_core)
    add(((0, tp), (1, tp_core)), True)
    taken(tp_far)
    taken(tp_other)
    for i in range(pieces):
        z_copy(theirs, i).wait_recv()
        other_copy(theirs, i).start()
    for i in range(pieces):
        other_copy(mine, i).wait_recv()
        other_copy(theirs, i).wait_recv()
    down_arrived(1)
    add(((2, tp_far), (3, tp_other)), False)

    def square(q, carry):
        cols = pl.ds(pl.multiple_of(q * step, step), step)
        mid = (res[:, cols].astype(f32) + total[:, cols]).astype(bf16)
        res[:, cols] = mid
        wide = mid.astype(f32)
        return carry + jnp.sum(wide * wide, axis=1, keepdims=True)

    sums = lax.fori_loop(0, width // step, square, jnp.zeros((block, 1), f32))
    scale = lax.rsqrt(sums / width + norm_eps)

    def spread_norm(q, carry):
        cols = pl.ds(pl.multiple_of(q * step, step), step)
        normed[:, cols] = (res[:, cols].astype(f32) * scale * gain[:, cols]).astype(bf16)
        return carry

    lax.fori_loop(0, width // step, spread_norm, 0)
    pl.when(has_right)(lambda: lead_copy(0).start())
    pl.when(has_left)(lambda: lead_copy(1).start())
    put_normed = pltpu.make_async_copy(normed, normed_out, l_sem.at[0])
    put_normed.start()
    for load in loads[4:]:
        load.wait()
    both = jnp.dot(normed[...], sgu[...], preferred_element_type=f32)
    hidden = (jax.nn.silu(both[:, :inner]) * both[:, inner:]).astype(bf16)

    def shared(q, carry):
        cols = pl.ds(pl.multiple_of(q * step, step), step)
        total[:, cols] = res[:, cols].astype(f32) + jnp.dot(hidden, sdown[:, cols], preferred_element_type=f32)
        return carry

    lax.fori_loop(0, width // step, shared, 0)
    put_base = pltpu.make_async_copy(total, base, l_sem.at[1])
    put_base.start()
    down_relayed(0)
    down_arrived(2)
    for p in range(1, far_early):
        down_relayed(p)
    for p in range(early):
        down_copy(1, p).wait_recv()
        if p < far_early:
            down_copy(3, p).wait_recv()
            down_copy(2, p).wait_send()
            down_copy(3, p).wait_send()
        down_copy(0, p).wait_send()
        down_copy(1, p).wait_send()
    pl.when(has_left)(lambda: lead_copy(0).wait_recv())
    pl.when(has_right)(lambda: lead_copy(1).wait_recv())
    pl.when(has_right)(lambda: lead_copy(0).wait_send())
    pl.when(has_left)(lambda: lead_copy(1).wait_send())
    put_normed.wait()
    put_base.wait()

    pl.when(has_next)(lambda: to_next().wait_send())
    pl.when(has_prev)(lambda: to_prev().wait_send())
    core_copy().wait_send()
    for i in range(pieces):
        far_copy(i).wait_send()
        z_copy(mine, i).wait_send()
        other_copy(mine, i).wait_send()
        other_copy(theirs, i).wait_send()
    for b in range(quarters):
        pl.when(tp != b)(lambda: block_copy(b).wait_send())


def mixer(pool_in, pool_weight, pool_scale, out_weight, resid, gain, shared_gate, shared_up, shared_down, down, ids, shares, experts):
    count = lax.axis_size("sp")
    quarters = lax.axis_size("tp")
    length = count // 2
    tok_local, group = pool_in.shape
    assert pool_weight.shape[0] == 1 and quarters == 4 and length % 2 == 0
    rows, width = resid.shape
    bf16, f32 = jnp.bfloat16, jnp.float32
    dma = pltpu.SemaphoreType.DMA
    pieces = 2
    deep = down.shape[0]
    inner = shared_gate.shape[1]
    anywhere = pl.BlockSpec(memory_space=pl.ANY)
    local = pl.BlockSpec(memory_space=pltpu.VMEM)
    return pl.pallas_call(
        functools.partial(mixer_kernel, length, experts),
        out_shape=[
            jax.ShapeDtypeStruct((rows, width), f32),
            jax.ShapeDtypeStruct((rows, width), bf16),
            jax.ShapeDtypeStruct((quarters, deep // quarters, width), bf16),
            jax.ShapeDtypeStruct((2, rows, width // 4), bf16),
            jax.ShapeDtypeStruct((rows, 128), bf16),
        ],
        in_specs=[anywhere, anywhere, local, anywhere, anywhere, local] + [anywhere] * 4 + [local] * 2,
        out_specs=[anywhere] * 4 + [local],
        scratch_shapes=[
            pltpu.VMEM((tok_local + 32, group), f32),
            pltpu.VMEM((2, 16, group), bf16),
            pltpu.VMEM((tok_local, group), bf16),
            pltpu.VMEM((group, group), bf16),
            pltpu.VMEM((quarters, rows, group), bf16),
            pltpu.VMEM((quarters, rows, group), bf16),
            pltpu.VMEM((quarters, group, width), bf16),
            pltpu.VMEM((rows, width), f32),
            pltpu.VMEM((rows, width), bf16),
            pltpu.VMEM((rows, width), bf16),
            pltpu.VMEM((width, 2 * inner), bf16),
            pltpu.VMEM((inner, width), bf16),
            dma((2,)), dma((2,)), dma((quarters,)), dma((quarters,)), dma((1,)), dma((1,)),
            dma((pieces,)), dma((pieces,)), dma((pieces,)), dma((pieces,)),
            dma((2, pieces)), dma((2, pieces)), dma((4, 4)), dma((4, 4)), dma((2,)), dma((2,)), dma((7,)),
        ],
        compiler_params=pltpu.CompilerParams(
            collective_id=1, has_side_effects=True, vmem_limit_bytes=56 * 2**20
        ),
        cost_estimate=pl.CostEstimate(flops=10**11, bytes_accessed=10**8, transcendentals=0),
    )(
        pool_in, pool_weight, pool_scale[None, :], out_weight, resid, gain[None, :],
        shared_gate, shared_up, shared_down, down, ids, shares,
    )


def moe_kernel(
    length, cap, quarters,
    x, mt, wdp_in, gate, up, down, base, lead,
    out, wdp, inbuf,
    xbuf, mbuf, wgu, wdbuf, xr, xp, ho, hsp, hits, hacc, hp, hr, m8, stage, total_out, out_stage,
    x_send, x_recv, m_send, m_recv, y_send, y_recv, h_send, h_recv, r_send, r_recv,
    wd_send, wd_recv, w_sem, s_sem, l_sem, own_sem,
):
    f32, bf16 = jnp.float32, jnp.bfloat16
    rows, width = x.shape
    local, _, inner = gate.shape
    deep = local * inner
    total = local * 2 * length
    rows_y = xr.shape[0]
    pieces = r_send.shape[1]
    piece = width // pieces
    chunk = wdbuf.shape[2]
    chunks = width // chunk
    part = wdp.shape[1]
    me = lax.axis_index("sp")
    tp = lax.axis_index("tp")
    spot, side = me // 2, me % 2
    mate = me + 1 - 2 * side
    tp_core = tp + 1 - 2 * (tp % 2)
    tp_far = (tp + quarters // 2) % quarters
    last = length - 1
    has_left, has_right = spot > 0, spot < last
    barrier = pltpu.get_barrier_semaphore()

    def greet(device):
        pl.semaphore_signal(barrier, inc=1, device_id=device, device_id_type=MESH)

    greet({"sp": mate})
    greet({"tp": tp_core})
    greet({"tp": tp_far})

    @pl.when(has_left)
    def _():
        greet({"sp": me - 2})

    @pl.when(has_right)
    def _():
        greet({"sp": me + 2})

    pl.semaphore_wait(barrier, 3 + jnp.minimum(spot, 1) + jnp.minimum(last - spot, 1))

    def remote(src, dst, send, recv, device):
        return pltpu.make_async_remote_copy(
            src_ref=src, dst_ref=dst, send_sem=send, recv_sem=recv, device_id=device, device_id_type=MESH
        )

    def cols_of(q):
        return pl.ds(pl.multiple_of(q * piece, piece), piece)

    def onward(way):
        return {"sp": me + 2} if way == 0 else {"sp": me - 2}

    def row_copy(way, source, q, src):
        cols = cols_of(q)
        return remote(
            src.at[:, cols], xbuf.at[source, :, cols], x_send.at[way, source, q], x_recv.at[source, q], onward(way)
        )

    def table_copy(way, source, src):
        return remote(src, mbuf.at[source], m_send.at[way, source], m_recv.at[source], onward(way))

    def each_piece(act, first=0):
        def one(q, carry):
            act(q)
            return carry

        lax.fori_loop(first, pieces, one, 0)

    def lead_load(way):
        source = spot - 1 if way == 0 else spot + 1
        return pltpu.make_async_copy(lead.at[way], xbuf.at[source, :, pl.ds(0, piece)], own_sem.at[3 + way])

    pl.when(has_left)(lambda: lead_load(0).start())
    pl.when(has_right)(lambda: lead_load(1).start())

    def send_own(way):
        table_copy(way, spot, mt).start()
        each_piece(lambda q: row_copy(way, spot, q, x).start(), 1)

    pl.when(has_right)(lambda: send_own(0))
    pl.when(has_left)(lambda: send_own(1))

    own_rows = pltpu.make_async_copy(x, xbuf.at[spot], own_sem.at[0])
    own_table = pltpu.make_async_copy(mt, mbuf.at[spot], own_sem.at[1])
    own_rows.start()
    own_table.start()

    d_pieces = wd_send.shape[1]
    d_piece = width // d_pieces
    end_piece = d_pieces - 1

    def quarter_copy(slot, p):
        cols = pl.ds(p * d_piece, d_piece)
        if slot == 0:
            src = down.at[pl.ds(pl.multiple_of(tp * part, 8), part), cols]
        else:
            src = wdp.at[2 if slot == 3 else 0, :, cols]
        device = ({"sp": mate}, {"tp": tp_core}, {"tp": tp_far}, {"tp": tp_core})[slot]
        return remote(src, wdp.at[slot, :, cols], wd_send.at[slot, p], wd_recv.at[slot, p], device)

    gate_load = pltpu.make_async_copy(gate, wgu.at[:, :, pl.ds(0, inner)], w_sem.at[0])
    up_load = pltpu.make_async_copy(up, wgu.at[:, :, pl.ds(inner, inner)], w_sem.at[1])
    gate_load.start()
    up_load.start()
    quarter_copy(0, end_piece).start()
    for p in range(1, end_piece):
        quarter_copy(2, p).start()
    base_load = pltpu.make_async_copy(base, total_out, own_sem.at[2])
    base_load.start()

    def source_of(j):
        close = jnp.minimum(spot, last - spot)
        near = jnp.where(j % 2 == 1, spot - (j + 1) // 2, spot + j // 2)
        far = jnp.where(spot < last - spot, spot + j - close, spot - (j - close))
        return jnp.where(j <= 2 * close, near, far)

    def take_piece(hop, q):
        def take(source, way, goes_on):
            leads = (hop == 1) & (q == 0)
            pl.when(leads)(lambda: lead_load(way).wait())
            pl.when(jnp.logical_not(leads))(lambda: row_copy(way, source, q, xbuf.at[source]).wait_recv())
            pl.when(goes_on)(lambda: row_copy(way, source, q, xbuf.at[source]).start())

            @pl.when(q == 0)
            def _():
                table_copy(way, source, mbuf.at[source]).wait_recv()
                pl.when(goes_on)(lambda: table_copy(way, source, mbuf.at[source]).start())

        pl.when(spot >= hop)(lambda: take(spot - hop, 0, has_right))
        pl.when(spot + hop <= last)(lambda: take(spot + hop, 1, has_left))

    def slot_hits(table, e):
        place = table[:, 5 * local + e : 5 * local + e + 1]
        columns = lax.broadcasted_iota(jnp.int32, (rows, rows_y), 1).astype(f32)
        return ((place >= 0.0) & (columns == place + float(cap * e))).astype(f32)

    def weight_of(table, i):
        return table[:, i : i + 1] + table[:, 2 * local + i : 2 * local + i + 1]

    def y_copy(j, q):
        cols = cols_of(q)
        return remote(xr.at[:, cols], xp.at[j % 2, :, cols], y_send.at[q], y_recv.at[j % 2, q], {"sp": mate})

    def h_copy(j):
        return remote(hp, hr.at[j], h_send.at[0], h_recv.at[j], {"sp": mate})

    def keep_table(j):
        c = lax.broadcasted_iota(jnp.int32, (128, 128), 1)
        group = (c >= 2 * local).astype(jnp.int32) + (c >= 4 * local).astype(jnp.int32)
        i = c - 2 * local * group
        expert = jnp.where(i < local, me * local + i, mate * local + i - local)
        choose = (lax.broadcasted_iota(jnp.int32, (128, 128), 0) == group * total + expert) & (c < 6 * local)
        m8[j] = jnp.dot(mbuf[source_of(j)], choose.astype(f32).astype(bf16), preferred_element_type=f32)

    def gather_piece(j, q):
        source = source_of(j)

        @pl.when(q == 0)
        def _():
            pl.when(j > 0)(lambda: keep_table(j))
            table = m8[j]
            found = slot_hits(table, 0)
            for e in range(1, local):
                found = found + slot_hits(table, e)
            hits[...] = found.astype(bf16)

        pl.when(j != 1)(lambda: y_copy(j, q).wait_send())
        cols = cols_of(q)
        xr[:, cols] = lax.dot_general(
            hits[...], xbuf[source, :, cols], (((0,), (0,)), ((), ())), preferred_element_type=f32
        ).astype(bf16)
        y_copy(j, q).start()

    def gated(lhs, e):
        both = jnp.dot(lhs, wgu[e], preferred_element_type=f32)
        return jax.nn.silu(both[:, :inner]) * both[:, inner:]

    def own_hidden(j, first, end):
        source = source_of(j)

        def one(e, carry):
            table = m8[j]
            lanes = lax.broadcasted_iota(jnp.int32, table.shape, 1)
            mine = jnp.where((lanes == e) | (lanes == 2 * local + e), table, 0.0)
            weight = jnp.sum(mine, axis=1, keepdims=True)
            cols = pl.ds(pl.multiple_of(e * inner, 128), inner)
            ho[jnp.minimum(j, 1), :, cols] = (gated(xbuf[source], e) * weight).astype(bf16)
            return carry

        lax.fori_loop(first, end, one, 0)

    cover = max(-(-(cap * (e + 1)) // 16) * 16 - cap * e // 16 * 16 for e in range(local))

    def mate_hidden(j):
        each_piece(lambda q: y_copy(j, q).wait_recv())
        hacc[...] = jnp.zeros_like(hacc)

        def one(e, carry):
            first = pl.multiple_of(cap * e // 16 * 16, 16)
            found = gated(xp[j % 2, pl.ds(first, cover), :], e)
            spots = lax.broadcasted_iota(jnp.int32, found.shape, 0) + first
            keep = (spots >= cap * e) & (spots < cap * (e + 1))
            hacc[pl.ds(first, cover), :] += jnp.where(keep, found, 0.0)
            return carry

        lax.fori_loop(0, local, one, 0)

        pl.when(j != 1)(lambda: h_copy(j).wait_send())
        hp[...] = hacc[...].astype(bf16)
        h_copy(j).start()

    def down_copies(c, slot):
        cols = pl.ds(pl.multiple_of(c * chunk, chunk), chunk)
        copies = [pltpu.make_async_copy(down.at[:, cols], wdbuf.at[slot, pl.ds(0, deep), :], s_sem.at[slot, 0])]
        where = (tp, tp_core, tp_far, tp + 3 - 2 * (tp % 2) - 2 * ((tp // 2) * 2))
        for n in range(quarters):
            src = wdp.at[n, :, cols]
            place = pl.ds(pl.multiple_of(deep + where[n] * part, 16), part)
            copies.append(pltpu.make_async_copy(src, wdbuf.at[slot, place, :], s_sem.at[slot, 1 + n]))
        return copies

    def load_down(c, slot):
        for copy in down_copies(c, slot):
            copy.start()

    def return_copy(way, source, q):
        cols = cols_of(q)
        target = jnp.where(spot + 1 == source, length, source) if way == 0 else source
        return remote(
            xbuf.at[source, :, cols], inbuf.at[target, :, cols], r_send.at[source, q], r_recv.at[target, q], onward(way)
        )

    def return_wait(slot, q):
        cols = cols_of(q)
        remote(
            xbuf.at[0, :, cols], inbuf.at[slot, :, cols], r_send.at[0, q], r_recv.at[slot, q], {"sp": mate}
        ).wait_recv()

    def scatter_hidden(j):
        table = m8[j]
        for e in range(local):
            spread = jnp.dot(slot_hits(table, e).astype(bf16), hr[j], preferred_element_type=f32)
            hsp[:, e * inner : (e + 1) * inner] = (spread * weight_of(table, local + e)).astype(bf16)

    ratio = chunks // pieces

    def down_chunk(j, c):
        slot = c % 2
        pl.when(c + 1 < chunks)(lambda: load_down(c + 1, 1 - slot))
        for copy in down_copies(c, slot):
            copy.wait()
        cols = pl.ds(pl.multiple_of(c * chunk, chunk), chunk)
        result = jnp.dot(ho[jnp.minimum(j, 1)], wdbuf[slot, :deep, :], preferred_element_type=f32)
        return cols, result + jnp.dot(hsp[...], wdbuf[slot, deep:, :], preferred_element_type=f32)

    def project(j, first, end):
        source = source_of(j)

        def one(c, carry):
            fresh = c % ratio == 0
            pl.when(fresh & (source < spot) & has_right)(
                lambda: row_copy(0, source, c // ratio, xbuf.at[source]).wait_send()
            )
            pl.when(fresh & (source > spot) & has_left)(
                lambda: row_copy(1, source, c // ratio, xbuf.at[source]).wait_send()
            )
            cols, result = down_chunk(j, c)
            xbuf[source, :, cols] = result.astype(bf16)
            whole = c % ratio == ratio - 1

            @pl.when(whole & (spot == last) & (source < spot))
            def _():
                return_copy(1, source, c // ratio).start()

            @pl.when(whole & (spot == 0) & (source > spot))
            def _():
                return_copy(0, source, c // ratio).start()

            return carry

        lax.fori_loop(first, end, one, 0)

    def project_own(first, end):
        def one(c, carry):
            cols, result = down_chunk(0, c)
            total_out[:, cols] += result
            return carry

        lax.fori_loop(first, end, one, 0)

    def fold(slot, q, n):
        cols = cols_of(q)
        if stage is None:
            return inbuf[slot, :, cols].astype(f32)
        copy = pltpu.make_async_copy(inbuf.at[slot, :, cols], stage.at[n], l_sem.at[n])
        copy.start()
        copy.wait()
        return stage[n].astype(f32)

    def relay(k, first, end):
        def hand_on(way, source, q):
            cols = cols_of(q)
            return_wait(source, q)
            both = xbuf[source, :, cols].astype(f32) + fold(source, q, way)
            xbuf[source, :, cols] = both.astype(bf16)
            return_copy(way, source, q).start()

        def one(tau, carry):
            left, right = tau - (last - spot), tau - spot

            @pl.when((spot > last - k) & has_right & (left >= 0) & (left < pieces))
            def _():
                hand_on(1, last - k, left)

            @pl.when((spot < k) & has_left & (right >= 0) & (right < pieces))
            def _():
                hand_on(0, k, right)

            return carry

        lax.fori_loop(first, end, one, 0)

    middle = chunks // 2

    def window(w, carry):
        j = w - 1
        pl.when(w >= 4)(lambda: relay(w - 2, 1, 2))
        pl.when(w >= 2)(lambda: own_hidden(j, 0, local))
        pl.when(w >= 4)(lambda: relay(w - 2, 2, 3))

        def one(q, inner_carry):
            @pl.when(w < length)
            def _():
                take_piece(w, q)
                gather_piece(w, q)

            @pl.when((w == 1) & (q == 0))
            def _():
                gate_load.wait()
                up_load.wait()
                own_hidden(0, 0, local)
                quarter_copy(0, end_piece).wait_recv()
                quarter_copy(1, end_piece).start()
                quarter_copy(2, end_piece).start()

            @pl.when((w >= 2) & (q == 0))
            def _():
                mate_hidden(j)

                @pl.when(w == 2)
                def _():
                    for p in range(1, end_piece):
                        quarter_copy(2, p).wait_recv()
                        quarter_copy(3, p).start()

                pl.when(w > 2)(lambda: load_down(0, 0))
                pl.when(w >= 4)(lambda: relay(w - 2, 3, 4))

            @pl.when((w >= 2) & (q == 1))
            def _():
                @pl.when(w == 2)
                def _():
                    for p in range(1, end_piece):
                        quarter_copy(3, p).wait_recv()
                    load_down(0, 0)

                h_copy(j).wait_recv()
                scatter_hidden(j)

            @pl.when((w == 2) & (q == 2))
            def _():
                quarter_copy(2, end_piece).wait_recv()
                quarter_copy(3, end_piece).start()
                quarter_copy(1, end_piece).wait_recv()
                quarter_copy(3, end_piece).wait_recv()

            @pl.when((w >= 2) & ((q == 1) | (q == 2)))
            def _():
                project(j, (q - 1) * middle, q * middle)

            pl.when((w >= 4) & (q == 1))(lambda: relay(w - 2, 4, pieces + last))
            pl.when((w == length) & (q == 1))(lambda: each_piece(lambda p: gather_piece(0, p)))
            return inner_carry

        return lax.fori_loop(0, pieces, one, carry)

    own_rows.wait()
    own_table.wait()
    keep_table(0)
    lax.fori_loop(1, length + 1, window, 0)
    relay(last, 1, 4)
    mate_hidden(0)
    load_down(0, 0)
    relay(last, 4, 5)
    h_copy(0).wait_recv()
    scatter_hidden(0)
    base_load.wait()
    project_own(0, middle)
    relay(last, 5, pieces + last)
    project_own(middle, chunks)

    def out_copy(q):
        cols = cols_of(q)
        return pltpu.make_async_copy(out_stage.at[:, cols], out.at[:, cols], s_sem.at[0, q])

    def finish(q, carry):
        cols = cols_of(q)

        @pl.when(has_right)
        def _():
            return_wait(spot, q)
            total_out[:, cols] += fold(spot, q, 0)

        @pl.when(has_left)
        def _():
            return_wait(length, q)
            total_out[:, cols] += fold(length, q, 1)

        out_stage[:, cols] = total_out[:, cols].astype(bf16)
        out_copy(q).start()
        return carry

    lax.fori_loop(0, pieces, finish, 0)
    each_piece(lambda q: out_copy(q).wait())

    each_piece(lambda q: y_copy(0, q).wait_send())
    h_copy(0).wait_send()
    for slot in (0, 1):
        quarter_copy(slot, end_piece).wait_send()
    for p in range(1, d_pieces):
        quarter_copy(2, p).wait_send()
        quarter_copy(3, p).wait_send()

    def drain_own(way):
        each_piece(lambda q: row_copy(way, spot, q, x).wait_send(), 1)

    pl.when(has_right)(lambda: drain_own(0))
    pl.when(has_left)(lambda: drain_own(1))

    def drain(s, carry):
        pl.when((s <= spot) & has_right)(lambda: table_copy(0, s, mbuf.at[s]).wait_send())
        pl.when((s >= spot) & has_left)(lambda: table_copy(1, s, mbuf.at[s]).wait_send())

        @pl.when(s != spot)
        def _():
            each_piece(lambda q: return_copy(1, s, q).wait_send())

        return carry

    lax.fori_loop(0, length, drain, 0)


def routed_experts(normed, mt, expert_gate, expert_up, expert_down, mate_down, base, lead):
    count = lax.axis_size("sp")
    quarters = lax.axis_size("tp")
    assert count % 2 == 0 and count >= 6 and quarters == 4
    length = count // 2
    local, _, inner = expert_gate.shape
    total = local * count
    rows, width = normed.shape
    pieces = 4
    piece = width // pieces
    chunk = piece // 2
    cap = expert_slots
    rows_y = -(-(cap * local) // 16) * 16
    deep = local * inner
    bf16, f32 = jnp.bfloat16, jnp.float32
    dma = pltpu.SemaphoreType.DMA
    anywhere = pl.BlockSpec(memory_space=pl.ANY)
    landing = (length + 1, rows, width)
    direct = 2 * math.prod(landing) < 12 * 2**20
    scratch = [
        pltpu.VMEM((length, rows, width), bf16),
        pltpu.VMEM((length, rows, 128), bf16),
        pltpu.VMEM((local, width, 2 * inner), bf16),
        pltpu.VMEM((2, 2 * deep, chunk), bf16),
        pltpu.VMEM((rows_y, width), bf16),
        pltpu.VMEM((2, rows_y, width), bf16),
        pltpu.VMEM((2, rows, deep), bf16),
        pltpu.VMEM((rows, deep), bf16),
        pltpu.VMEM((rows, rows_y), bf16),
        pltpu.VMEM((rows_y, inner), f32),
        pltpu.VMEM((rows_y, inner), bf16),
        pltpu.VMEM((length, rows_y, inner), bf16),
        pltpu.VMEM((length, rows, 128), f32),
        None if direct else pltpu.VMEM((2, rows, piece), bf16),
        pltpu.VMEM((rows, width), f32),
        pltpu.VMEM((rows, width), bf16),
        dma((2, length, pieces)), dma((length, pieces)), dma((2, length)), dma((length,)),
        dma((pieces,)), dma((2, pieces)), dma((1,)), dma((length,)),
        dma((length, pieces)), dma((length + 1, pieces)),
        dma((4, 4)), dma((4, 4)), dma((2,)), dma((2, 1 + quarters)), dma((2,)), dma((5,)),
    ]
    outs = [
        jax.ShapeDtypeStruct((rows, width), bf16),
        jax.ShapeDtypeStruct((quarters, deep // quarters, width), bf16),
    ]
    kernel = functools.partial(moe_kernel, length, cap, quarters)
    if direct:
        scratch.insert(0, pltpu.VMEM(landing, bf16))
        gap = 10 + 1 + 13
        scratch.remove(None)

        def body(*refs):
            return kernel(*refs[:gap], None, *refs[gap:])
    else:
        outs.append(jax.ShapeDtypeStruct(landing, bf16))
        body = kernel
    results = pl.pallas_call(
        body,
        out_shape=outs,
        in_specs=[anywhere] * 8,
        out_specs=[anywhere] * len(outs),
        input_output_aliases={2: 1},
        scratch_shapes=scratch,
        compiler_params=pltpu.CompilerParams(
            collective_id=0, has_side_effects=True, vmem_limit_bytes=67043328
        ),
    )(normed, mt, mate_down, expert_gate, expert_up, expert_down.reshape(deep, width), base, lead)
    return results[0]


def shards(
    resid,
    pool_in,
    pool_weight,
    pool_scale,
    out_weight,
    norm_gain,
    route_ids,
    route_weight,
    expert_gate,
    expert_up,
    expert_down,
    shared_gate,
    shared_up,
    shared_down,
):
    flat_down = expert_down.reshape(-1, expert_down.shape[2])
    experts = expert_gate.shape[0] * lax.axis_size("sp")
    assert 3 * experts <= 128
    base, normed, mate_down, lead, mt = mixer(
        pool_in, pool_weight, pool_scale, out_weight, resid, norm_gain,
        shared_gate, shared_up, shared_down, flat_down, route_ids.T, route_weight.T, experts,
    )
    return routed_experts(normed, mt, expert_gate, expert_up, expert_down, mate_down, base, lead)


def solution(mesh):
    return jax.shard_map(
        shards,
        mesh=mesh,
        in_specs=(
            P(("sp", "tp"), None),
            P("sp", "tp"),
            P("tp", None, None),
            P("tp"),
            P("tp", None),
            P(),
            P(("sp", "tp"), None),
            P(("sp", "tp"), None),
            P("sp", None, None),
            P("sp", None, None),
            P("sp", None, None),
            P(),
            P(),
            P(),
        ),
        out_specs=P(("sp", "tp"), None),
        check_vma=False,
    )
```
